32 devices in a mesh: grp: 2 (over x), ep: 8 (over z, y), tp: 2 (over core).
Axes of the slice: x: 2, y: 2, z: 4, core: 2. Of those that a mesh axis runs over, the one named last changes fastest.
Arguments:
- tokens: bfloat16 [512, 2048], P(('grp', 'ep')), parts along dimension 0, may hold values from -6 to 6
- norm_gain: float32 [2048], replicated, may hold values from 0.1 to 1.9
- group_prob: float32 [512], P(('grp', 'ep')), parts along dimension 0, may hold values from 0.5 to 1
- route_logits: float32 [512, 4], P(('grp', 'ep')), parts along dimension 0, may hold values from -6 to 6
- expert_ids: int32 [512, 4], P(('grp', 'ep')), parts along dimension 0, may hold values from 0 to 7, as said below
- w_gate: bfloat16 [8, 2048, 512], P('ep', None, 'tp'), may hold values from -0.125 to 0.125
- w_up: bfloat16 [8, 2048, 512], P('ep', None, 'tp'), may hold values from -0.125 to 0.125
- w_down: bfloat16 [8, 512, 2048], P('ep', 'tp'), may hold values from -0.25 to 0.25
Outputs:
- mixed: bfloat16 [512, 2048], P(('grp', 'ep')), parts along dimension 0
The draws below stay inside these ranges and needn't reach their ends.
There are 2 independent parts, one for each index of `grp`. The reference program is written for one: setup_inputs(seed, part) draws one part's arguments, and reference() takes and returns one part's arrays. A program takes and returns all parts, laid end to end along the dimension named above; an argument that names none is the same for every part. Nothing has to cross between parts.
Inputs may be any that keep to these rules, and one draw needn't show every extreme that they name: `expert_ids`: each token names 4 different experts, all inside one group of 4 consecutive experts. Of the 32 tokens of one index of ep, exactly 16 lie in each group, so at most 16 of them name any one expert; in every draw some expert is named by 16 tokens of every index of ep.
All inputs are finite; a program needn't handle non-finite values.
Results may differ from the reference program's by a relative error of at most 0.0077.
Values may be sent and summed in bfloat16 or wider, within the bound.
A program may use at most 64 MiB of HBM per device.

```python
import jax
import jax.numpy as jnp
from jax import lax

D = 2048
FF = 512
GROUPS = 2
TOP_K = 4
TOK_DEV = 32
EXPERTS = 8
GROUP_SIZE = 4
TOKENS = 256
N_TP = 2


def draw_expert_ids(key, part):
    blocks = TOKENS // TOK_DEV
    keys = jax.random.split(jax.random.fold_in(key, 7), 5)
    labels = jnp.arange(TOK_DEV, dtype=jnp.int32) % GROUPS
    perms = jax.vmap(lambda k: jax.random.permutation(k, labels))(jax.random.split(keys[0], blocks))
    common_hot = jax.random.randint(keys[1], (), 0, GROUP_SIZE)
    hot = jax.random.randint(keys[2], (blocks, GROUPS), 0, GROUP_SIZE)
    hot = hot.at[:, 0].set(common_hot)
    bias = jax.random.randint(keys[3], (GROUPS, GROUP_SIZE), 0, 4) * 32
    noise = jax.random.randint(keys[4], (blocks, TOK_DEV, GROUP_SIZE), 0, 64)
    local = jnp.arange(GROUP_SIZE, dtype=jnp.int32)
    token_bias = bias[perms]
    token_hot = jnp.take_along_axis(hot, perms, axis=1)
    boost = (local[None, None, :] == token_hot[:, :, None]).astype(jnp.int32) * 100000
    scores = (noise + token_bias + boost) * GROUP_SIZE + local[None, None, :]
    unused, picked = lax.top_k(scores, TOP_K)
    ids = perms[:, :, None] * GROUP_SIZE + picked.astype(jnp.int32)
    return ids.reshape(TOKENS, TOP_K).astype(jnp.int32)


def levels(own_key, shape, pieces, low, largest):
    factor_of, own = 1.0, jax.random.fold_in(own_key, 6)
    for position, shards_of in pieces:
        heights = jnp.exp(jax.random.uniform(jax.random.fold_in(own, position), (shards_of,), jnp.float32, low / len(pieces), largest / len(pieces)))
        factor_of = factor_of * jnp.repeat(heights, shape[position] // shards_of).reshape([-1 if axis == position else 1 for axis in range(len(shape))])
    return factor_of


def normal_values(rng, dims, deviation, limit, cuts=(), held_as=jnp.bfloat16):
    factor_of = levels(rng, dims, cuts, -0.22, 0.18) if cuts else 1.0
    drawn = jax.random.normal(rng, dims, jnp.float32) * deviation * factor_of
    return jnp.minimum(jnp.maximum(drawn, -limit), limit).astype(held_as)


def setup_inputs(seed: int = 0, part: int = 0) -> dict:
    arg_keys = jax.random.split(jax.random.key(seed), 9)
    part_keys = jax.random.split(jax.random.fold_in(arg_keys[8], part), 9)
    return {
        "tokens": normal_values(part_keys[0], (TOKENS, D), 1.0, 6.0, ((0, 8),)),
        "norm_gain": jnp.clip(1.0 + 0.18 * jax.random.normal(arg_keys[1], (D,), jnp.float32), 0.1, 1.9),
        "group_prob": jnp.clip(0.5 + 0.5 * jax.random.uniform(part_keys[2], (TOKENS,), jnp.float32) ** levels(part_keys[2], (TOKENS,), ((0, 8),), -0.2, 0.2), 0.5, 1.0),
        "route_logits": normal_values(part_keys[3], (TOKENS, TOP_K), 1.0, 6.0, ((0, 8),), jnp.float32),
        "expert_ids": draw_expert_ids(jax.random.fold_in(jax.random.fold_in(arg_keys[8], part), 71), part),
        "w_gate": normal_values(arg_keys[5], (EXPERTS, D, FF), D ** -0.5, 0.125, ((0, 8), (2, 2))),
        "w_up": normal_values(arg_keys[6], (EXPERTS, D, FF), D ** -0.5, 0.125, ((0, 8), (2, 2))),
        "w_down": normal_values(arg_keys[7], (EXPERTS, FF, D), FF ** -0.5, 0.25, ((0, 8), (1, 2))),
    }


def reference(tokens, norm_gain, group_prob, route_logits, expert_ids, w_gate, w_up, w_down):
    values = tokens.astype(jnp.float32)
    scale = lax.rsqrt(lax.optimization_barrier(jnp.mean(values * values, axis=-1, keepdims=True)) + 1e-06)
    normed = (values * scale * norm_gain).astype(jnp.bfloat16)
    expw = jnp.exp(route_logits)
    route_w = group_prob[:, None] * expw / lax.optimization_barrier(jnp.sum(expw, axis=-1, keepdims=True))
    block = FF // N_TP

    def one_expert(acc, inputs):
        gate_m, up_m, down_m, index = inputs
        gate = jnp.dot(normed, gate_m, preferred_element_type=jnp.float32)
        up = jnp.dot(normed, up_m, preferred_element_type=jnp.float32)
        act = (jax.nn.silu(gate) * up).astype(jnp.bfloat16)
        total = jnp.zeros((normed.shape[0], normed.shape[1]), jnp.float32)
        for piece in range(N_TP):
            part = jnp.dot(act[:, piece * block:(piece + 1) * block], down_m[piece * block:(piece + 1) * block], preferred_element_type=jnp.float32).astype(jnp.bfloat16)
            total = total + lax.optimization_barrier(part).astype(jnp.float32)
        expert_out = lax.optimization_barrier(total.astype(jnp.bfloat16)).astype(jnp.float32)
        weight = lax.optimization_barrier(jnp.sum(route_w * (expert_ids == index).astype(jnp.float32), axis=1))
        return (acc + weight[:, None] * expert_out, None)
    start = jnp.zeros((normed.shape[0], normed.shape[1]), jnp.float32)
    experts = jnp.arange(EXPERTS, dtype=jnp.int32)
    acc, unused = lax.scan(one_expert, start, (w_gate, w_up, w_down, experts))
    return acc.astype(jnp.bfloat16)
```

```python
import functools

import jax
import jax.numpy as jnp
from jax import lax
from jax.experimental import pallas as pl
from jax.experimental.pallas import tpu as pltpu
from jax.sharding import PartitionSpec as P

GROUPS = 2
CHUNKS = 4
MESH = pl.DeviceIdType.MESH


def kernel(
    width, n_tp,
    tok_hbm, gain_hbm, prob_hbm, logit_hbm, ids_hbm, wg_hbm, wu_hbm, wd_hbm,
    out_ref,
    tok, gain, prob, logit, ids, wg, wu, wd, send, wsend, wroot, x, outs, back, red, mixed,
    in_sem, wl_sem, ws_sem, wr_sem, xs_sem, xr_sem, vs_sem, vr_sem,
    ds_sem, dr_sem, bs_sem, br_sem, cs_sem, cr_sem, ms_sem, mr_sem,
):
    e = lax.axis_index("ep")
    q = lax.axis_index("tp")
    sib = n_tp - 1 - q
    gs = width // GROUPS
    count, dmodel = tok.shape
    cap = count // GROUPS
    topk = ids.shape[0]
    block = e // gs
    local = e % gs
    base = block * gs
    partner = (e + gs) % width
    cross = q == n_tp - 1
    own = q != n_tp - 1
    group = (block + q) % GROUPS
    cw = dmodel // CHUNKS
    f32, bf = jnp.float32, jnp.bfloat16

    def cols(c):
        return pl.ds(c * cw, cw)

    def peer(j):
        return base + (local + j) % gs

    def remote(src, dst, ss, rs, **where):
        return pltpu.make_async_remote_copy(
            src_ref=src, dst_ref=dst, send_sem=ss, recv_sem=rs,
            device_id=where, device_id_type=MESH,
        )

    smalls = [
        pltpu.make_async_copy(src, dst, in_sem.at[i])
        for i, (src, dst) in enumerate(
            [(tok_hbm, tok), (gain_hbm, gain), (prob_hbm, prob), (logit_hbm, logit), (ids_hbm, ids)]
        )
    ]
    for c in smalls:
        c.start()
    weights = [(wg_hbm, wg), (wu_hbm, wu), (wd_hbm, wd)]
    loads = [
        pltpu.make_async_copy(src.at[0], dst.at[q], wl_sem.at[i]) for i, (src, dst) in enumerate(weights)
    ]
    for c in loads:
        c.start()

    barrier = pltpu.get_barrier_semaphore()

    @pl.when(cross)
    def _():
        pl.semaphore_signal(barrier, inc=1, device_id={"ep": partner}, device_id_type=MESH)

    for j in range(1, gs):
        pl.semaphore_signal(barrier, inc=1, device_id={"ep": peer(j)}, device_id_type=MESH)
    pl.semaphore_signal(barrier, inc=1, device_id={"tp": sib}, device_id_type=MESH)

    for c in smalls:
        c.wait()
    values = tok[...].astype(f32)
    scale = lax.rsqrt(jnp.mean(values * values, axis=-1, keepdims=True) + 1e-06)
    normed = (values * scale * gain[...]).astype(bf)
    idv = ids[...]
    first = idv[0:1, :]
    grow = jnp.zeros((1, count), f32)
    for g in range(1, GROUPS):
        grow = grow + jnp.where(first >= g * gs, 1.0, 0.0)
    t_row = lax.broadcasted_iota(jnp.int32, (count, count), 0)
    t_col = lax.broadcasted_iota(jnp.int32, (count, count), 1)
    gfull = jnp.broadcast_to(grow, (count, count))
    gcol = jnp.sum(jnp.where(t_row == t_col, gfull, 0.0), axis=1, keepdims=True)
    same = jnp.where(gfull == gcol, 1.0, 0.0)
    pos_row = jnp.sum(jnp.where(t_row < t_col, same, 0.0), axis=0, keepdims=True)
    pos_col = jnp.sum(jnp.where(t_col < t_row, same, 0.0), axis=1, keepdims=True)
    r_io = lax.broadcasted_iota(jnp.int32, (cap, count), 0).astype(f32)
    place = jnp.where((pos_row == r_io) & (grow == group.astype(f32)), 1.0, 0.0)
    rows = jnp.dot(place.astype(bf), normed, preferred_element_type=f32).astype(bf)

    @pl.when(cross)
    def _():
        send[...] = rows

    @pl.when(own)
    def _():
        x[0] = rows

    pl.semaphore_wait(barrier, jnp.where(cross, gs + 1, gs))

    def across(c):
        return remote(send.at[:, cols(c)], x.at[0, :, cols(c)], xs_sem.at[c], xr_sem.at[c], ep=partner)

    def spread(j, c):
        return remote(
            x.at[0, :, cols(c)], x.at[j, :, cols(c)], ds_sem.at[j, c], dr_sem.at[j, c], ep=peer(j)
        )

    @pl.when(cross)
    def _():
        for c in range(CHUNKS):
            across(c).start()

    @pl.when(own)
    def _():
        for c in range(CHUNKS):
            for j in range(1, gs):
                spread(j, c).start()

    def swap(i, c):
        ref = weights[i][1]
        part = ref.at[q, cols(c)] if i < 2 else ref.at[q, :, cols(c)]
        return remote(part, part, ws_sem.at[i, c], wr_sem.at[i, c], tp=sib)

    def swapped(i, c):
        ref = weights[i][1]
        part = ref.at[sib, cols(c)] if i < 2 else ref.at[sib, :, cols(c)]
        return remote(part, part, ws_sem.at[i, c], wr_sem.at[i, c], tp=sib)

    loads[0].wait()
    loads[1].wait()
    for c in range(CHUNKS):
        for i in range(2):
            swap(i, c).start()
    loads[2].wait()
    for c in range(CHUNKS):
        swap(2, c).start()

    expw = jnp.exp(logit[...])
    route = prob[...] * expw / jnp.sum(expw, axis=0, keepdims=True)
    k_io = lax.broadcasted_iota(jnp.int32, (128, count), 0)
    expert = jnp.where(k_io < gs, group * gs + lax.rem(k_io + local, gs), -1)
    wtok = jnp.zeros((128, count), f32)
    for k in range(topk):
        wtok = wtok + jnp.where(idv[k : k + 1, :] == expert, route[k : k + 1, :], 0.0)
    wslot = lax.dot_general(
        place, wtok, (((1,), (1,)), ((), ())),
        precision=lax.Precision.HIGHEST, preferred_element_type=f32,
    )

    def weights_across():
        return remote(wsend, wroot, vs_sem, vr_sem, ep=partner)

    @pl.when(cross)
    def _():
        wsend[...] = wslot
        weights_across().start()

    @pl.when(own)
    def _():
        wroot[...] = wslot

    s_io = lax.broadcasted_iota(jnp.int32, (count, count), 1).astype(f32)
    role = jnp.where(gcol == block.astype(f32), 0.0, 1.0)
    unplace = jnp.where(s_io == role * cap + pos_col, 1.0, 0.0).astype(bf)

    @pl.when(cross)
    def _():
        for c in range(CHUNKS):
            across(c).wait_recv()
            for j in range(1, gs):
                spread(j, c).start()

    gates = [jnp.zeros((gs * cap, wg.shape[2]), f32)] * n_tp
    ups = [jnp.zeros((gs * cap, wu.shape[2]), f32)] * n_tp
    for c in range(CHUNKS):
        for i in range(2):
            swapped(i, c).wait_recv()
        for j in range(1, gs):
            spread(j, c).wait_recv()
        xc = x[:, :, c * cw : (c + 1) * cw].reshape(gs * cap, cw)
        for h in range(n_tp):
            gates[h] = gates[h] + jnp.dot(xc, wg[h, c * cw : (c + 1) * cw], preferred_element_type=f32)
            ups[h] = ups[h] + jnp.dot(xc, wu[h, c * cw : (c + 1) * cw], preferred_element_type=f32)
    acts = [((g / (1.0 + jnp.exp(-g))) * u).astype(bf) for g, u in zip(gates, ups)]

    def give(j, c):
        return remote(
            outs.at[j, :, cols(c)], back.at[j, :, cols(c)], bs_sem.at[j, c], br_sem.at[j, c],
            ep=base + (local + gs - j) % gs,
        )

    for c in range(CHUNKS):
        swapped(2, c).wait_recv()
        total = jnp.dot(acts[0], wd[0, :, c * cw : (c + 1) * cw], preferred_element_type=f32)
        for h in range(1, n_tp):
            total = total + jnp.dot(acts[h], wd[h, :, c * cw : (c + 1) * cw], preferred_element_type=f32)
        outs[:, :, c * cw : (c + 1) * cw] = total.astype(bf).reshape(gs, cap, cw)
        for j in range(1, gs):
            give(j, c).start()

    def home(c):
        return remote(
            red.at[:, cols(c)], mixed.at[n_tp - 1, :, cols(c)], cs_sem.at[c], cr_sem.at[c], ep=partner
        )

    def share(c):
        part = mixed.at[q, :, cols(c)]
        return remote(part, part, ms_sem.at[c], mr_sem.at[c], tp=sib)

    def shared(c):
        part = mixed.at[sib, :, cols(c)]
        return remote(part, part, ms_sem.at[c], mr_sem.at[c], tp=sib)

    @pl.when(cross)
    def _():
        weights_across().wait_recv()

    wv = wroot[...]
    for c in range(CHUNKS):
        acc = wv[:, 0:1] * outs[0, :, c * cw : (c + 1) * cw].astype(f32)
        for j in range(1, gs):
            give(j, c).wait_recv()
            acc = acc + wv[:, j : j + 1] * back[j, :, c * cw : (c + 1) * cw].astype(f32)
        done = acc.astype(bf)

        @pl.when(cross)
        def _():
            red[:, c * cw : (c + 1) * cw] = done
            home(c).start()

        @pl.when(own)
        def _():
            mixed[0, :, c * cw : (c + 1) * cw] = done
            share(c).start()

    @pl.when(cross)
    def _():
        for c in range(CHUNKS):
            home(c).wait_recv()
            share(c).start()

    for c in range(CHUNKS):
        shared(c).wait_recv()
        slots = mixed[:, :, c * cw : (c + 1) * cw].reshape(count, cw)
        out_ref[:, c * cw : (c + 1) * cw] = jnp.dot(unplace, slots, preferred_element_type=f32).astype(bf)

    @pl.when(cross)
    def _():
        weights_across().wait_send()
        for c in range(CHUNKS):
            across(c).wait_send()
            home(c).wait_send()

    for c in range(CHUNKS):
        for i in range(3):
            swap(i, c).wait_send()
        for j in range(1, gs):
            spread(j, c).wait_send()
            give(j, c).wait_send()
        share(c).wait_send()


def shards(tokens, norm_gain, group_prob, route_logits, expert_ids, w_gate, w_up, w_down):
    width = lax.axis_size("ep")
    n_tp = lax.axis_size("tp")
    count, dmodel = tokens.shape
    topk = expert_ids.shape[1]
    ff = w_gate.shape[2]
    cap = count // GROUPS
    gs = width // GROUPS
    hbm = pl.BlockSpec(memory_space=pltpu.HBM)
    bf, f32 = jnp.bfloat16, jnp.float32
    dma = pltpu.SemaphoreType.DMA
    return pl.pallas_call(
        functools.partial(kernel, width, n_tp),
        out_shape=pltpu.VMEM((count, dmodel), bf),
        in_specs=[hbm] * 8,
        out_specs=pl.BlockSpec(memory_space=pltpu.VMEM),
        scratch_shapes=[
            pltpu.VMEM((count, dmodel), bf),
            pltpu.VMEM((1, dmodel), f32),
            pltpu.VMEM((1, count), f32),
            pltpu.VMEM((topk, count), f32),
            pltpu.VMEM((topk, count), jnp.int32),
            pltpu.VMEM((n_tp, dmodel, ff), bf),
            pltpu.VMEM((n_tp, dmodel, ff), bf),
            pltpu.VMEM((n_tp, ff, dmodel), bf),
            pltpu.VMEM((cap, dmodel), bf),
            pltpu.VMEM((cap, 128), f32),
            pltpu.VMEM((cap, 128), f32),
            pltpu.VMEM((gs, cap, dmodel), bf),
            pltpu.VMEM((gs, cap, dmodel), bf),
            pltpu.VMEM((gs, cap, dmodel), bf),
            pltpu.VMEM((cap, dmodel), bf),
            pltpu.VMEM((n_tp, cap, dmodel), bf),
            dma((5,)), dma((3,)), dma((3, CHUNKS)), dma((3, CHUNKS)),
            dma((CHUNKS,)), dma((CHUNKS,)), dma, dma,
            dma((gs, CHUNKS)), dma((gs, CHUNKS)), dma((gs, CHUNKS)), dma((gs, CHUNKS)),
            dma((CHUNKS,)), dma((CHUNKS,)), dma((CHUNKS,)), dma((CHUNKS,)),
        ],
        compiler_params=pltpu.CompilerParams(collective_id=0, has_side_effects=True),
        name="expert_mixture",
    )(
        tokens, norm_gain.reshape(1, dmodel), group_prob.reshape(1, count), route_logits.T,
        expert_ids.T, w_gate, w_up, w_down,
    )


def solution(mesh):
    in_specs = (
        P(("grp", "ep"), None),
        P(),
        P(("grp", "ep")),
        P(("grp", "ep"), None),
        P(("grp", "ep"), None),
        P("ep", None, "tp"),
        P("ep", None, "tp"),
        P("ep", "tp", None),
    )
    out_specs = P(("grp", "ep"), None)
    return jax.shard_map(shards, mesh=mesh, in_specs=in_specs, out_specs=out_specs, check_vma=False)
```

```python
import functools

import jax
import jax.numpy as jnp
from jax import lax
from jax.experimental import pallas as pl
from jax.experimental.pallas import tpu as pltpu
from jax.sharding import PartitionSpec as P

GROUPS = 2
CHUNKS = 4
FIRST = 1
MESH = pl.DeviceIdType.MESH


def kernel(
    width, n_tp,
    tok_hbm, gain_hbm, prob_hbm, logit_hbm, ids_hbm, wg_hbm, wu_hbm, wd_hbm,
    out_ref,
    tok, gain, prob, logit, ids, wi, wd, send, wsend, wroot, x, outs, back, red, mixed,
    in_sem, wl_sem, ws_sem, wr_sem, xs_sem, xr_sem, vs_sem, vr_sem,
    ds_sem, dr_sem, bs_sem, br_sem, cs_sem, cr_sem, ms_sem, mr_sem,
):
    e = lax.axis_index("ep")
    q = lax.axis_index("tp")
    sib = n_tp - 1 - q
    gs = width // GROUPS
    count, dmodel = tok.shape
    cap = count // GROUPS
    topk = ids.shape[0]
    block = e // gs
    local = e % gs
    base = block * gs
    partner = (e + gs) % width
    cross = q == n_tp - 1
    own = q != n_tp - 1
    group = (block + q) % GROUPS
    cw = dmodel // CHUNKS
    ff = wi.shape[3]
    f32, bf = jnp.float32, jnp.bfloat16
    batches = [(0, FIRST), (FIRST, gs)]

    def cols(c):
        return pl.ds(c * cw, cw)

    def peer(j):
        return base + (local + j) % gs

    def remote(src, dst, ss, rs, **where):
        return pltpu.make_async_remote_copy(
            src_ref=src, dst_ref=dst, send_sem=ss, recv_sem=rs,
            device_id=where, device_id_type=MESH,
        )

    smalls = [
        pltpu.make_async_copy(src, dst, in_sem.at[i])
        for i, (src, dst) in enumerate(
            [(tok_hbm, tok), (gain_hbm, gain), (prob_hbm, prob), (logit_hbm, logit), (ids_hbm, ids)]
        )
    ]
    for c in smalls:
        c.start()
    loads = [
        pltpu.make_async_copy(src.at[0], dst, wl_sem.at[i])
        for i, (src, dst) in enumerate([(wg_hbm, wi.at[0, q]), (wu_hbm, wi.at[1, q]), (wd_hbm, wd.at[q])])
    ]
    for c in loads:
        c.start()

    barrier = pltpu.get_barrier_semaphore()

    @pl.when(cross)
    def _():
        pl.semaphore_signal(barrier, inc=1, device_id={"ep": partner}, device_id_type=MESH)

    for j in range(1, gs):
        pl.semaphore_signal(barrier, inc=1, device_id={"ep": peer(j)}, device_id_type=MESH)
    pl.semaphore_signal(barrier, inc=1, device_id={"tp": sib}, device_id_type=MESH)

    for c in smalls:
        c.wait()
    values = tok[...].astype(f32)
    scale = lax.rsqrt(jnp.mean(values * values, axis=-1, keepdims=True) + 1e-06)
    normed = (values * scale * gain[...]).astype(bf)
    idv = ids[...]
    first = idv[0:1, :]
    grow = jnp.zeros((1, count), f32)
    for g in range(1, GROUPS):
        grow = grow + jnp.where(first >= g * gs, 1.0, 0.0)
    t_row = lax.broadcasted_iota(jnp.int32, (count, count), 0)
    t_col = lax.broadcasted_iota(jnp.int32, (count, count), 1)
    gfull = jnp.broadcast_to(grow, (count, count))
    gcol = jnp.sum(jnp.where(t_row == t_col, gfull, 0.0), axis=1, keepdims=True)
    same = jnp.where(gfull == gcol, 1.0, 0.0)
    pos_row = jnp.sum(jnp.where(t_row < t_col, same, 0.0), axis=0, keepdims=True)
    pos_col = jnp.sum(jnp.where(t_col < t_row, same, 0.0), axis=1, keepdims=True)
    r_io = lax.broadcasted_iota(jnp.int32, (cap, count), 0).astype(f32)
    place = jnp.where((pos_row == r_io) & (grow == group.astype(f32)), 1.0, 0.0)
    rows = jnp.dot(place.astype(bf), normed, preferred_element_type=f32).astype(bf)

    @pl.when(cross)
    def _():
        send[...] = rows

    @pl.when(own)
    def _():
        x[local] = rows

    pl.semaphore_wait(barrier, jnp.where(cross, gs + 1, gs))

    def across(c):
        return remote(send.at[:, cols(c)], x.at[local, :, cols(c)], xs_sem, xr_sem.at[c], ep=partner)

    def spread(j, c):
        part = x.at[local, :, cols(c)]
        return remote(part, part, ds_sem, dr_sem.at[jnp.where(local < FIRST, 0, 1), c], ep=peer(j))

    @pl.when(cross)
    def _():
        for c in range(CHUNKS):
            across(c).start()

    @pl.when(own)
    def _():
        for c in range(CHUNKS):
            for j in range(1, gs):
                spread(j, c).start()

    def swap(src, dst, i):
        return remote(src, dst, ws_sem.at[i], wr_sem.at[i], tp=sib)

    for i in range(2):
        loads[i].wait()
        swap(wi.at[i, q], wi.at[i, q], 0).start()
    loads[2].wait()
    swap(wd.at[q], wd.at[q], 1).start()

    expw = jnp.exp(logit[...])
    route = prob[...] * expw / jnp.sum(expw, axis=0, keepdims=True)
    expert = lax.broadcasted_iota(jnp.int32, (128, count), 0) + group * gs
    wtok = jnp.zeros((128, count), f32)
    for k in range(topk):
        wtok = wtok + jnp.where(idv[k : k + 1, :] == expert, route[k : k + 1, :], 0.0)
    wslot = lax.dot_general(
        place, wtok, (((1,), (1,)), ((), ())),
        precision=lax.Precision.HIGHEST, preferred_element_type=f32,
    )

    def weights_across():
        return remote(wsend, wroot, vs_sem, vr_sem, ep=partner)

    @pl.when(cross)
    def _():
        wsend[...] = wslot
        weights_across().start()

    @pl.when(own)
    def _():
        wroot[...] = wslot

    s_io = lax.broadcasted_iota(jnp.int32, (count, count), 1).astype(f32)
    role = jnp.where(gcol == block.astype(f32), 0.0, 1.0)
    unplace = jnp.where(s_io == role * cap + pos_col, 1.0, 0.0).astype(bf)

    @pl.when(cross)
    def _():
        for c in range(CHUNKS):
            across(c).wait_recv()
            for j in range(1, gs):
                spread(j, c).start()

    def landed(b, c):
        lo, hi = batches[b]
        inside = (local >= lo) & (local < hi)

        def take(n):
            part = x.at[pl.ds(lo, n), :, cols(c)]
            remote(part, part, ds_sem, dr_sem.at[b, c], tp=sib).wait_recv()

        if hi - lo > 1:

            @pl.when(inside)
            def _():
                take(hi - lo - 1)

        @pl.when(jnp.logical_not(inside))
        def _():
            take(hi - lo)

    def give(r, c):
        return remote(
            outs.at[r, :, cols(c)], back.at[local, :, cols(c)], bs_sem, br_sem.at[c], ep=base + r
        )

    for b, (lo, hi) in enumerate(batches):
        n = (hi - lo) * cap
        gates = [jnp.zeros((n, ff), f32)] * n_tp
        ups = [jnp.zeros((n, ff), f32)] * n_tp
        for c in range(CHUNKS):
            landed(b, c)
            if b == 0 and c == 0:
                swap(wi.at[:, sib], wi.at[:, sib], 0).wait_recv()
            k = slice(c * cw, (c + 1) * cw)
            xc = x[lo:hi, :, k].reshape(n, cw)
            for h in range(n_tp):
                gates[h] = gates[h] + jnp.dot(xc, wi[0, h, k], preferred_element_type=f32)
                ups[h] = ups[h] + jnp.dot(xc, wi[1, h, k], preferred_element_type=f32)
        acts = [((g / (1.0 + jnp.exp(-g))) * u).astype(bf) for g, u in zip(gates, ups)]
        if b == 0:
            swap(wd.at[sib], wd.at[sib], 1).wait_recv()
        for c in range(CHUNKS):
            k = slice(c * cw, (c + 1) * cw)
            total = jnp.dot(acts[0], wd[0, :, k], preferred_element_type=f32)
            for h in range(1, n_tp):
                total = total + jnp.dot(acts[h], wd[h, :, k], preferred_element_type=f32)
            outs[lo:hi, :, k] = total.astype(bf).reshape(hi - lo, cap, cw)
            for r in range(lo, hi):

                @pl.when(local == r)
                def _():
                    back[r, :, k] = outs[r, :, k]

                @pl.when(local != r)
                def _():
                    give(r, c).start()

    def home(c):
        return remote(
            red.at[:, cols(c)], mixed.at[n_tp - 1, :, cols(c)], cs_sem, cr_sem.at[c], ep=partner
        )

    def share(c):
        part = mixed.at[q, :, cols(c)]
        return remote(part, part, ms_sem, mr_sem.at[c], tp=sib)

    def shared(c):
        part = mixed.at[sib, :, cols(c)]
        return remote(part, part, ms_sem, mr_sem.at[c], tp=sib)

    @pl.when(cross)
    def _():
        weights_across().wait_recv()

    wv = wroot[...]
    for c in range(CHUNKS):
        part = back.at[pl.ds(0, gs - 1), :, cols(c)]
        remote(part, part, bs_sem, br_sem.at[c], tp=sib).wait_recv()
        k = slice(c * cw, (c + 1) * cw)
        acc = wv[:, 0:1] * back[0, :, k].astype(f32)
        for j in range(1, gs):
            acc = acc + wv[:, j : j + 1] * back[j, :, k].astype(f32)
        done = acc.astype(bf)

        @pl.when(cross)
        def _():
            red[:, k] = done
            home(c).start()

        @pl.when(own)
        def _():
            mixed[0, :, k] = done
            share(c).start()

    @pl.when(cross)
    def _():
        for c in range(CHUNKS):
            home(c).wait_recv()
            share(c).start()

    for c in range(CHUNKS):
        shared(c).wait_recv()
        k = slice(c * cw, (c + 1) * cw)
        slots = mixed[:, :, k].reshape(count, cw)
        out_ref[:, k] = jnp.dot(unplace, slots, preferred_element_type=f32).astype(bf)

    @pl.when(cross)
    def _():
        weights_across().wait_send()
        remote(send, send, xs_sem, xr_sem.at[0], tp=sib).wait_send()
        remote(red, red, cs_sem, cr_sem.at[0], tp=sib).wait_send()

    swap(wi.at[:, q], wi.at[:, q], 0).wait_send()
    swap(wd.at[q], wd.at[q], 1).wait_send()
    most = x.at[pl.ds(0, gs - 1)]
    remote(most, most, ds_sem, dr_sem.at[0, 0], tp=sib).wait_send()
    remote(most, most, bs_sem, br_sem.at[0], tp=sib).wait_send()
    remote(mixed.at[q], mixed.at[q], ms_sem, mr_sem.at[0], tp=sib).wait_send()


def shards(tokens, norm_gain, group_prob, route_logits, expert_ids, w_gate, w_up, w_down):
    width = lax.axis_size("ep")
    n_tp = lax.axis_size("tp")
    count, dmodel = tokens.shape
    topk = expert_ids.shape[1]
    ff = w_gate.shape[2]
    cap = count // GROUPS
    gs = width // GROUPS
    hbm = pl.BlockSpec(memory_space=pltpu.HBM)
    bf, f32 = jnp.bfloat16, jnp.float32
    dma = pltpu.SemaphoreType.DMA
    return pl.pallas_call(
        functools.partial(kernel, width, n_tp),
        out_shape=pltpu.VMEM((count, dmodel), bf),
        in_specs=[hbm] * 8,
        out_specs=pl.BlockSpec(memory_space=pltpu.VMEM),
        scratch_shapes=[
            pltpu.VMEM((count, dmodel), bf),
            pltpu.VMEM((1, dmodel), f32),
            pltpu.VMEM((1, count), f32),
            pltpu.VMEM((topk, count), f32),
            pltpu.VMEM((topk, count), jnp.int32),
            pltpu.VMEM((2, n_tp, dmodel, ff), bf),
            pltpu.VMEM((n_tp, ff, dmodel), bf),
            pltpu.VMEM((cap, dmodel), bf),
            pltpu.VMEM((cap, 128), f32),
            pltpu.VMEM((cap, 128), f32),
            pltpu.VMEM((gs, cap, dmodel), bf),
            pltpu.VMEM((gs, cap, dmodel), bf),
            pltpu.VMEM((gs, cap, dmodel), bf),
            pltpu.VMEM((cap, dmodel), bf),
            pltpu.VMEM((n_tp, cap, dmodel), bf),
            dma((5,)), dma((3,)), dma((2,)), dma((2,)),
            dma, dma((CHUNKS,)), dma, dma,
            dma, dma((2, CHUNKS)), dma, dma((CHUNKS,)),
            dma, dma((CHUNKS,)), dma, dma((CHUNKS,)),
        ],
        compiler_params=pltpu.CompilerParams(collective_id=0, has_side_effects=True),
        name="expert_mixture",
    )(
        tokens, norm_gain.reshape(1, dmodel), group_prob.reshape(1, count), route_logits.T,
        expert_ids.T, w_gate, w_up, w_down,
    )


def solution(mesh):
    in_specs = (
        P(("grp", "ep"), None),
        P(),
        P(("grp", "ep")),
        P(("grp", "ep"), None),
        P(("grp", "ep"), None),
        P("ep", None, "tp"),
        P("ep", None, "tp"),
        P("ep", "tp", None),
    )
    out_specs = P(("grp", "ep"), None)
    return jax.shard_map(shards, mesh=mesh, in_specs=in_specs, out_specs=out_specs, check_vma=False)
```

```python
import functools

import jax
import jax.numpy as jnp
from jax import lax
from jax.experimental import pallas as pl
from jax.experimental.pallas import tpu as pltpu
from jax.sharding import PartitionSpec as P

GROUPS = 2
CHUNKS = 4
FIRST = 1
HOLD = 2
MESH = pl.DeviceIdType.MESH


def kernel(
    width, n_tp,
    tok_hbm, gain_hbm, prob_hbm, logit_hbm, ids_hbm, wg_hbm, wu_hbm, wd_hbm,
    out_ref,
    tok, gain, prob, logit, ids, wi, wd, send, wsend, wroot, x, outs, back, red, mixed,
    in_sem, wl_sem, ws_sem, wr_sem, xs_sem, xr_sem, vs_sem, vr_sem,
    ds_sem, dr_sem, bs_sem, br_sem, cs_sem, cr_sem, ms_sem, mr_sem,
):
    e = lax.axis_index("ep")
    q = lax.axis_index("tp")
    sib = n_tp - 1 - q
    gs = width // GROUPS
    count, dmodel = tok.shape
    cap = count // GROUPS
    topk = ids.shape[0]
    block = e // gs
    local = e % gs
    base = block * gs
    partner = (e + gs) % width
    cross = q == n_tp - 1
    own = q != n_tp - 1
    group = (block + q) % GROUPS
    cw = dmodel // CHUNKS
    ff = wi.shape[3]
    f32, bf = jnp.float32, jnp.bfloat16
    batches = [(0, FIRST), (FIRST, gs)]

    def cols(c):
        return pl.ds(c * cw, cw)

    def peer(j):
        return base + (local + j) % gs

    def remote(src, dst, ss, rs, **where):
        return pltpu.make_async_remote_copy(
            src_ref=src, dst_ref=dst, send_sem=ss, recv_sem=rs,
            device_id=where, device_id_type=MESH,
        )

    smalls = [
        pltpu.make_async_copy(src, dst, in_sem.at[i])
        for i, (src, dst) in enumerate(
            [(tok_hbm, tok), (gain_hbm, gain), (prob_hbm, prob), (logit_hbm, logit), (ids_hbm, ids)]
        )
    ]
    for c in smalls:
        c.start()
    loads = [
        pltpu.make_async_copy(src.at[0], dst, wl_sem.at[i])
        for i, (src, dst) in enumerate([(wg_hbm, wi.at[0, q]), (wu_hbm, wi.at[1, q]), (wd_hbm, wd.at[q])])
    ]
    for c in loads:
        c.start()

    barrier = pltpu.get_barrier_semaphore()

    @pl.when(cross)
    def _():
        pl.semaphore_signal(barrier, inc=1, device_id={"ep": partner}, device_id_type=MESH)

    for j in range(1, gs):
        pl.semaphore_signal(barrier, inc=1, device_id={"ep": peer(j)}, device_id_type=MESH)
    pl.semaphore_signal(barrier, inc=1, device_id={"tp": sib}, device_id_type=MESH)

    for c in smalls:
        c.wait()
    values = tok[...].astype(f32)
    scale = lax.rsqrt(jnp.mean(values * values, axis=-1, keepdims=True) + 1e-06)
    normed = (values * scale * gain[...]).astype(bf)
    idv = ids[...]
    first = idv[0:1, :]
    grow = jnp.zeros((1, count), f32)
    for g in range(1, GROUPS):
        grow = grow + jnp.where(first >= g * gs, 1.0, 0.0)
    t_row = lax.broadcasted_iota(jnp.int32, (count, count), 0)
    t_col = lax.broadcasted_iota(jnp.int32, (count, count), 1)
    gfull = jnp.broadcast_to(grow, (count, count))
    gcol = jnp.sum(jnp.where(t_row == t_col, gfull, 0.0), axis=1, keepdims=True)
    same = jnp.where(gfull == gcol, 1.0, 0.0)
    pos_row = jnp.sum(jnp.where(t_row < t_col, same, 0.0), axis=0, keepdims=True)
    pos_col = jnp.sum(jnp.where(t_col < t_row, same, 0.0), axis=1, keepdims=True)
    r_io = lax.broadcasted_iota(jnp.int32, (cap, count), 0).astype(f32)
    place = jnp.where((pos_row == r_io) & (grow == group.astype(f32)), 1.0, 0.0)
    rows = jnp.dot(place.astype(bf), normed, preferred_element_type=f32).astype(bf)

    @pl.when(cross)
    def _():
        send[...] = rows

    @pl.when(own)
    def _():
        x[local] = rows

    pl.semaphore_wait(barrier, jnp.where(cross, gs + 1, gs))

    def across(c):
        return remote(send.at[:, cols(c)], x.at[local, :, cols(c)], xs_sem, xr_sem.at[c], ep=partner)

    def spread(j, c):
        part = x.at[local, :, cols(c)]
        return remote(part, part, ds_sem, dr_sem.at[jnp.where(local < FIRST, 0, 1), c], ep=peer(j))

    @pl.when(cross)
    def _():
        for c in range(CHUNKS):
            across(c).start()

    def spread_all():
        for c in range(CHUNKS):
            for j in range(1, gs):
                spread(j, c).start()

    @pl.when(own & (block == 0))
    def _():
        spread_all()

    def swap_in(h, c):
        part = wi.at[:, h, cols(c)]
        return remote(part, part, ws_sem.at[0], wr_sem.at[c], tp=sib)

    def swap_down(h, c):
        part = wd.at[h, :, cols(c)]
        return remote(part, part, ws_sem.at[1], wr_sem.at[CHUNKS + c], tp=sib)

    for c in loads[:2]:
        c.wait()
    for c in range(CHUNKS):
        swap_in(q, c).start()
    loads[2].wait()
    for c in range(CHUNKS):
        swap_down(q, c).start()

    expw = jnp.exp(logit[...])
    route = prob[...] * expw / jnp.sum(expw, axis=0, keepdims=True)
    expert = lax.broadcasted_iota(jnp.int32, (128, count), 0) + group * gs
    wtok = jnp.zeros((128, count), f32)
    for k in range(topk):
        wtok = wtok + jnp.where(idv[k : k + 1, :] == expert, route[k : k + 1, :], 0.0)
    wslot = lax.dot_general(
        place, wtok, (((1,), (1,)), ((), ())),
        precision=lax.Precision.HIGHEST, preferred_element_type=f32,
    )

    def weights_across():
        return remote(wsend, wroot, vs_sem, vr_sem, ep=partner)

    @pl.when(cross)
    def _():
        wsend[...] = wslot
        weights_across().start()

    @pl.when(own)
    def _():
        wroot[...] = wslot

    s_io = lax.broadcasted_iota(jnp.int32, (count, count), 1).astype(f32)
    role = jnp.where(gcol == block.astype(f32), 0.0, 1.0)
    unplace = jnp.where(s_io == role * cap + pos_col, 1.0, 0.0).astype(bf)

    late = own & (block != 0)

    @pl.when(late)
    def _():
        for c in range(HOLD):
            swap_in(sib, c).wait_recv()
        spread_all()

    @pl.when(cross)
    def _():
        for c in range(CHUNKS):
            across(c).wait_recv()
            for j in range(1, gs):
                spread(j, c).start()

    def landed(b, c):
        lo, hi = batches[b]
        inside = (local >= lo) & (local < hi)

        def take(n):
            part = x.at[pl.ds(lo, n), :, cols(c)]
            remote(part, part, ds_sem, dr_sem.at[b, c], tp=sib).wait_recv()

        if hi - lo > 1:

            @pl.when(inside)
            def _():
                take(hi - lo - 1)

        @pl.when(jnp.logical_not(inside))
        def _():
            take(hi - lo)

    def give(r, c):
        return remote(
            outs.at[r, :, cols(c)], back.at[local, :, cols(c)], bs_sem, br_sem.at[c], ep=base + r
        )

    for b, (lo, hi) in enumerate(batches):
        n = (hi - lo) * cap
        gates = [jnp.zeros((n, ff), f32)] * n_tp
        ups = [jnp.zeros((n, ff), f32)] * n_tp
        for c in range(CHUNKS):
            landed(b, c)
            if b == 0 and c >= HOLD:
                swap_in(sib, c).wait_recv()
            elif b == 0:

                @pl.when(jnp.logical_not(late))
                def _():
                    swap_in(sib, c).wait_recv()

            k = slice(c * cw, (c + 1) * cw)
            xc = x[lo:hi, :, k].reshape(n, cw)
            for h in range(n_tp):
                gates[h] = gates[h] + jnp.dot(xc, wi[0, h, k], preferred_element_type=f32)
                ups[h] = ups[h] + jnp.dot(xc, wi[1, h, k], preferred_element_type=f32)
        acts = [((g / (1.0 + jnp.exp(-g))) * u).astype(bf) for g, u in zip(gates, ups)]

        def down(c):
            if b == 0:
                swap_down(sib, c).wait_recv()
            k = slice(c * cw, (c + 1) * cw)
            total = jnp.dot(acts[0], wd[0, :, k], preferred_element_type=f32)
            for h in range(1, n_tp):
                total = total + jnp.dot(acts[h], wd[h, :, k], preferred_element_type=f32)
            return total.astype(bf).reshape(hi - lo, cap, cw)

        ready = down(0)
        for c in range(CHUNKS):
            k = slice(c * cw, (c + 1) * cw)
            outs[lo:hi, :, k] = ready
            if c + 1 < CHUNKS:
                ready = down(c + 1)
            for r in range(lo, hi):

                @pl.when(local == r)
                def _():
                    back[r, :, k] = outs[r, :, k]

                @pl.when(local != r)
                def _():
                    give(r, c).start()

    def home(c):
        return remote(
            red.at[:, cols(c)], mixed.at[n_tp - 1, :, cols(c)], cs_sem, cr_sem.at[c], ep=partner
        )

    def share(c):
        part = mixed.at[q, :, cols(c)]
        return remote(part, part, ms_sem, mr_sem.at[c], tp=sib)

    def shared(c):
        part = mixed.at[sib, :, cols(c)]
        return remote(part, part, ms_sem, mr_sem.at[c], tp=sib)

    @pl.when(cross)
    def _():
        weights_across().wait_recv()

    wv = wroot[...]
    for c in range(CHUNKS):
        part = back.at[pl.ds(0, gs - 1), :, cols(c)]
        remote(part, part, bs_sem, br_sem.at[c], tp=sib).wait_recv()
        k = slice(c * cw, (c + 1) * cw)
        acc = wv[:, 0:1] * back[0, :, k].astype(f32)
        for j in range(1, gs):
            acc = acc + wv[:, j : j + 1] * back[j, :, k].astype(f32)
        done = acc.astype(bf)

        @pl.when(cross)
        def _():
            red[:, k] = done
            home(c).start()

        @pl.when(own)
        def _():
            mixed[0, :, k] = done
            share(c).start()

    @pl.when(cross)
    def _():
        for c in range(CHUNKS):
            home(c).wait_recv()
            share(c).start()

    for c in range(CHUNKS):
        shared(c).wait_recv()
        k = slice(c * cw, (c + 1) * cw)
        slots = mixed[:, :, k].reshape(count, cw)
        out_ref[:, k] = jnp.dot(unplace, slots, preferred_element_type=f32).astype(bf)

    @pl.when(cross)
    def _():
        weights_across().wait_send()
        remote(send, send, xs_sem, xr_sem.at[0], tp=sib).wait_send()
        remote(red, red, cs_sem, cr_sem.at[0], tp=sib).wait_send()

    half_in, half_down = wi.at[:, q], wd.at[q]
    remote(half_in, half_in, ws_sem.at[0], wr_sem.at[0], tp=sib).wait_send()
    remote(half_down, half_down, ws_sem.at[1], wr_sem.at[0], tp=sib).wait_send()
    most = x.at[pl.ds(0, gs - 1)]
    remote(most, most, ds_sem, dr_sem.at[0, 0], tp=sib).wait_send()
    remote(most, most, bs_sem, br_sem.at[0], tp=sib).wait_send()
    remote(mixed.at[q], mixed.at[q], ms_sem, mr_sem.at[0], tp=sib).wait_send()


def shards(tokens, norm_gain, group_prob, route_logits, expert_ids, w_gate, w_up, w_down):
    width = lax.axis_size("ep")
    n_tp = lax.axis_size("tp")
    count, dmodel = tokens.shape
    topk = expert_ids.shape[1]
    ff = w_gate.shape[2]
    cap = count // GROUPS
    gs = width // GROUPS
    hbm = pl.BlockSpec(memory_space=pltpu.HBM)
    bf, f32 = jnp.bfloat16, jnp.float32
    dma = pltpu.SemaphoreType.DMA
    return pl.pallas_call(
        functools.partial(kernel, width, n_tp),
        out_shape=pltpu.VMEM((count, dmodel), bf),
        in_specs=[hbm] * 8,
        out_specs=pl.BlockSpec(memory_space=pltpu.VMEM),
        scratch_shapes=[
            pltpu.VMEM((count, dmodel), bf),
            pltpu.VMEM((1, dmodel), f32),
            pltpu.VMEM((1, count), f32),
            pltpu.VMEM((topk, count), f32),
            pltpu.VMEM((topk, count), jnp.int32),
            pltpu.VMEM((2, n_tp, dmodel, ff), bf),
            pltpu.VMEM((n_tp, ff, dmodel), bf),
            pltpu.VMEM((cap, dmodel), bf),
            pltpu.VMEM((cap, 128), f32),
            pltpu.VMEM((cap, 128), f32),
            pltpu.VMEM((gs, cap, dmodel), bf),
            pltpu.VMEM((gs, cap, dmodel), bf),
            pltpu.VMEM((gs, cap, dmodel), bf),
            pltpu.VMEM((cap, dmodel), bf),
            pltpu.VMEM((n_tp, cap, dmodel), bf),
            dma((5,)), dma((3,)), dma((2,)), dma((2 * CHUNKS,)),
            dma, dma((CHUNKS,)), dma, dma,
            dma, dma((2, CHUNKS)), dma, dma((CHUNKS,)),
            dma, dma((CHUNKS,)), dma, dma((CHUNKS,)),
        ],
        compiler_params=pltpu.CompilerParams(collective_id=0, has_side_effects=True),
        name="expert_mixture",
    )(
        tokens, norm_gain.reshape(1, dmodel), group_prob.reshape(1, count), route_logits.T,
        expert_ids.T, w_gate, w_up, w_down,
    )


def solution(mesh):
    in_specs = (
        P(("grp", "ep"), None),
        P(),
        P(("grp", "ep")),
        P(("grp", "ep"), None),
        P(("grp", "ep"), None),
        P("ep", None, "tp"),
        P("ep", None, "tp"),
        P("ep", "tp", None),
    )
    out_specs = P(("grp", "ep"), None)
    return jax.shard_map(shards, mesh=mesh, in_specs=in_specs, out_specs=out_specs, check_vma=False)
```

```python
import functools

import jax
import jax.numpy as jnp
from jax import lax
from jax.experimental import pallas as pl
from jax.experimental.pallas import tpu as pltpu
from jax.sharding import PartitionSpec as P

GROUPS = 2
CHUNKS = 4
FIRST = 1
HOLD = 3
MESH = pl.DeviceIdType.MESH


def kernel(
    width, n_tp,
    tok_hbm, gain_hbm, prob_hbm, logit_hbm, ids_hbm, wg_hbm, wu_hbm, wd_hbm,
    out_ref,
    tok, gain, prob, logit, ids, wi, wd, send, wsend, wroot, x, outs, back, red, got, mixed,
    in_sem, wl_sem, ws_sem, wr_sem, xs_sem, xr_sem, vs_sem, vr_sem,
    ds_sem, dr_sem, bs_sem, br_sem, cs_sem, cr_sem, ms_sem, mr_sem,
):
    e = lax.axis_index("ep")
    q = lax.axis_index("tp")
    sib = n_tp - 1 - q
    gs = width // GROUPS
    count, dmodel = tok.shape
    cap = count // GROUPS
    topk = ids.shape[0]
    block = e // gs
    local = e % gs
    base = block * gs
    partner = (e + gs) % width
    far = gs - 1 - local
    cross = q == n_tp - 1
    own = q != n_tp - 1
    group = (block + q) % GROUPS
    cw = dmodel // CHUNKS
    ff = wi.shape[3]
    f32, bf = jnp.float32, jnp.bfloat16
    split = cross & (block != 0)

    def cols(c):
        return pl.ds(c * cw, cw)

    def peer(j):
        return base + (local + j) % gs

    def remote(src, dst, ss, rs, **where):
        return pltpu.make_async_remote_copy(
            src_ref=src, dst_ref=dst, send_sem=ss, recv_sem=rs,
            device_id=where, device_id_type=MESH,
        )

    smalls = [
        pltpu.make_async_copy(src, dst, in_sem.at[i])
        for i, (src, dst) in enumerate(
            [(tok_hbm, tok), (gain_hbm, gain), (prob_hbm, prob), (logit_hbm, logit), (ids_hbm, ids)]
        )
    ]
    for c in smalls:
        c.start()
    loads = [
        pltpu.make_async_copy(src.at[0], dst, wl_sem.at[i])
        for i, (src, dst) in enumerate([(wg_hbm, wi.at[0, q]), (wu_hbm, wi.at[1, q]), (wd_hbm, wd.at[q])])
    ]
    for c in loads:
        c.start()

    barrier = pltpu.get_barrier_semaphore()

    @pl.when(cross)
    def _():
        pl.semaphore_signal(barrier, inc=1, device_id={"ep": partner}, device_id_type=MESH)

    for j in range(1, gs):
        pl.semaphore_signal(barrier, inc=1, device_id={"ep": peer(j)}, device_id_type=MESH)
    pl.semaphore_signal(barrier, inc=1, device_id={"tp": sib}, device_id_type=MESH)

    for c in smalls:
        c.wait()
    values = tok[...].astype(f32)
    scale = lax.rsqrt(jnp.mean(values * values, axis=-1, keepdims=True) + 1e-06)
    normed = (values * scale * gain[...]).astype(bf)
    idv = ids[...]
    first = idv[0:1, :]
    grow = jnp.zeros((1, count), f32)
    for g in range(1, GROUPS):
        grow = grow + jnp.where(first >= g * gs, 1.0, 0.0)
    t_row = lax.broadcasted_iota(jnp.int32, (count, count), 0)
    t_col = lax.broadcasted_iota(jnp.int32, (count, count), 1)
    gfull = jnp.broadcast_to(grow, (count, count))
    gcol = jnp.sum(jnp.where(t_row == t_col, gfull, 0.0), axis=1, keepdims=True)
    same = jnp.where(gfull == gcol, 1.0, 0.0)
    pos_row = jnp.sum(jnp.where(t_row < t_col, same, 0.0), axis=0, keepdims=True)
    pos_col = jnp.sum(jnp.where(t_col < t_row, same, 0.0), axis=1, keepdims=True)
    r_io = lax.broadcasted_iota(jnp.int32, (cap, count), 0).astype(f32)
    place = jnp.where((pos_row == r_io) & (grow == group.astype(f32)), 1.0, 0.0)
    rows = jnp.dot(place.astype(bf), normed, preferred_element_type=f32).astype(bf)

    @pl.when(cross)
    def _():
        send[...] = rows

    @pl.when(own)
    def _():
        x[local] = rows

    pl.semaphore_wait(barrier, jnp.where(cross, gs + 1, gs))

    def across(c):
        return remote(send.at[:, cols(c)], x.at[local, :, cols(c)], xs_sem, xr_sem.at[c], ep=partner)

    def spread(j, c):
        part = x.at[local, :, cols(c)]
        return remote(part, part, ds_sem, dr_sem.at[jnp.where(split & (local >= FIRST), 1, 0), c], ep=peer(j))

    @pl.when(cross)
    def _():
        for c in range(CHUNKS):
            across(c).start()

    def spread_all():
        for c in range(CHUNKS):
            for j in range(1, gs):
                spread(j, c).start()

    @pl.when(own & (block == 0))
    def _():
        spread_all()

    def swap_in(h, c):
        part = wi.at[:, h, cols(c)]
        return remote(part, part, ws_sem.at[0], wr_sem.at[c], tp=sib)

    def swap_down(h, c):
        part = wd.at[h, :, cols(c)]
        return remote(part, part, ws_sem.at[1], wr_sem.at[CHUNKS + c], tp=sib)

    for c in loads[:2]:
        c.wait()
    for c in range(CHUNKS):
        swap_in(q, c).start()
    loads[2].wait()
    for c in range(CHUNKS):
        swap_down(q, c).start()

    expw = jnp.exp(logit[...])
    route = prob[...] * expw / jnp.sum(expw, axis=0, keepdims=True)
    k_io = lax.broadcasted_iota(jnp.int32, (128, count), 0)
    column = jnp.where(k_io < gs - 1, k_io + jnp.where(k_io >= far, 1, 0), far)
    expert = jnp.where(k_io < gs, column + group * gs, -1)
    wtok = jnp.zeros((128, count), f32)
    for k in range(topk):
        wtok = wtok + jnp.where(idv[k : k + 1, :] == expert, route[k : k + 1, :], 0.0)
    wslot = lax.dot_general(
        place, wtok, (((1,), (1,)), ((), ())),
        precision=lax.Precision.HIGHEST, preferred_element_type=f32,
    )

    def weights_across():
        return remote(wsend, wroot, vs_sem, vr_sem, ep=partner)

    wsend[...] = wslot

    @pl.when(cross)
    def _():
        weights_across().start()

    s_io = lax.broadcasted_iota(jnp.int32, (count, count), 1).astype(f32)
    role = jnp.where(gcol == block.astype(f32), 0.0, 1.0)
    unplace = jnp.where(s_io == role * cap + pos_col, 1.0, 0.0).astype(bf)

    late = own & (block != 0)

    @pl.when(late)
    def _():
        for c in range(HOLD):
            swap_in(sib, c).wait_recv()
        spread_all()

    @pl.when(cross)
    def _():
        for c in range(CHUNKS):
            across(c).wait_recv()
            for j in range(1, gs):
                spread(j, c).start()

    def landed(b, lo, hi, c):
        inside = (local >= lo) & (local < hi)

        def take(n):
            part = x.at[pl.ds(lo, n), :, cols(c)]
            remote(part, part, ds_sem, dr_sem.at[b, c], tp=sib).wait_recv()

        if hi - lo == gs:
            take(gs - 1)
            return
        if hi - lo > 1:

            @pl.when(inside)
            def _():
                take(hi - lo - 1)

        @pl.when(jnp.logical_not(inside))
        def _():
            take(hi - lo)

    def give(r, c):
        return remote(
            outs.at[r, :, cols(c)], back.at[local, :, cols(c)], bs_sem, br_sem.at[c], ep=base + r
        )

    def direct(r, c):
        return remote(
            outs.at[r, :, cols(c)], got.at[1, :, cols(c)], bs_sem, cr_sem.at[c],
            ep=(base + r + gs) % width,
        )

    def experts(b, lo, hi):
        n = (hi - lo) * cap
        gates = [jnp.zeros((n, ff), f32)] * n_tp
        ups = [jnp.zeros((n, ff), f32)] * n_tp
        for c in range(CHUNKS):
            landed(b, lo, hi, c)
            if b == 0 and c >= HOLD:
                swap_in(sib, c).wait_recv()
            elif b == 0:

                @pl.when(jnp.logical_not(late))
                def _():
                    swap_in(sib, c).wait_recv()

            k = slice(c * cw, (c + 1) * cw)
            xc = x[lo:hi, :, k].reshape(n, cw)
            for h in range(n_tp):
                gates[h] = gates[h] + jnp.dot(xc, wi[0, h, k], preferred_element_type=f32)
                ups[h] = ups[h] + jnp.dot(xc, wi[1, h, k], preferred_element_type=f32)
        acts = [((g / (1.0 + jnp.exp(-g))) * u).astype(bf) for g, u in zip(gates, ups)]

        def down(c):
            if b == 0:
                swap_down(sib, c).wait_recv()
            k = slice(c * cw, (c + 1) * cw)
            total = jnp.dot(acts[0], wd[0, :, k], preferred_element_type=f32)
            for h in range(1, n_tp):
                total = total + jnp.dot(acts[h], wd[h, :, k], preferred_element_type=f32)
            return total.astype(bf).reshape(hi - lo, cap, cw)

        ready = down(0)
        for c in range(CHUNKS):
            k = slice(c * cw, (c + 1) * cw)
            outs[lo:hi, :, k] = ready
            if c + 1 < CHUNKS:
                ready = down(c + 1)
            for r in range(lo, hi):

                @pl.when(local == r)
                def _():
                    back[r, :, k] = outs[r, :, k]

                @pl.when((local != r) & (own | (far != r)))
                def _():
                    give(r, c).start()

                @pl.when(cross & (far == r))
                def _():
                    direct(r, c).start()

    @pl.when(split)
    def _():
        experts(0, 0, FIRST)
        experts(1, FIRST, gs)

    @pl.when(jnp.logical_not(split))
    def _():
        experts(0, 0, gs)

    def home(c):
        return remote(
            red.at[:, cols(c)], got.at[0, :, cols(c)], cs_sem, cr_sem.at[c], ep=partner
        )

    def share(c):
        part = mixed.at[q, :, cols(c)]
        return remote(part, part, ms_sem, mr_sem.at[c], tp=sib)

    def shared(c):
        part = mixed.at[sib, :, cols(c)]
        return remote(part, part, ms_sem, mr_sem.at[c], tp=sib)

    @pl.when(cross)
    def _():
        weights_across().wait_recv()

    wv = jnp.where(cross, wroot[...], wsend[...])
    near = [i + jnp.where(i >= far, 1, 0) for i in range(gs - 1)]
    for c in range(CHUNKS):
        k = slice(c * cw, (c + 1) * cw)

        def returned(n):
            part = back.at[pl.ds(0, n), :, cols(c)]
            remote(part, part, bs_sem, br_sem.at[c], tp=sib).wait_recv()

        @pl.when(cross)
        def _():
            returned(gs - 2)

        @pl.when(own)
        def _():
            returned(gs - 1)

        acc = wv[:, 0:1] * back[near[0], :, k].astype(f32)
        for i in range(1, gs - 1):
            acc = acc + wv[:, i : i + 1] * back[near[i], :, k].astype(f32)

        @pl.when(cross)
        def _():
            red[:, k] = acc.astype(bf)
            home(c).start()

        @pl.when(own)
        def _():
            last = wv[:, gs - 1 : gs] * back[far, :, k].astype(f32)
            mixed[0, :, k] = (acc + last).astype(bf)
            share(c).start()

    @pl.when(cross)
    def _():
        for c in range(CHUNKS):
            k = slice(c * cw, (c + 1) * cw)
            part = got.at[:, :, cols(c)]
            remote(part, part, cs_sem, cr_sem.at[c], tp=sib).wait_recv()
            last = wsend[:, gs - 1 : gs] * got[1, :, k].astype(f32)
            mixed[n_tp - 1, :, k] = (got[0, :, k].astype(f32) + last).astype(bf)
            share(c).start()

    for c in range(CHUNKS):
        k = slice(c * cw, (c + 1) * cw)
        shared(c).wait_recv()
        slots = mixed[:, :, k].reshape(count, cw)
        out_ref[:, k] = jnp.dot(unplace, slots, preferred_element_type=f32).astype(bf)

    @pl.when(cross)
    def _():
        weights_across().wait_send()
        remote(send, send, xs_sem, xr_sem.at[0], tp=sib).wait_send()
        remote(red, red, cs_sem, cr_sem.at[0], tp=sib).wait_send()

    half_in, half_down = wi.at[:, q], wd.at[q]
    remote(half_in, half_in, ws_sem.at[0], wr_sem.at[0], tp=sib).wait_send()
    remote(half_down, half_down, ws_sem.at[1], wr_sem.at[0], tp=sib).wait_send()
    most = x.at[pl.ds(0, gs - 1)]
    remote(most, most, ds_sem, dr_sem.at[0, 0], tp=sib).wait_send()
    remote(most, most, bs_sem, br_sem.at[0], tp=sib).wait_send()
    remote(mixed.at[q], mixed.at[q], ms_sem, mr_sem.at[0], tp=sib).wait_send()


def shards(tokens, norm_gain, group_prob, route_logits, expert_ids, w_gate, w_up, w_down):
    width = lax.axis_size("ep")
    n_tp = lax.axis_size("tp")
    count, dmodel = tokens.shape
    topk = expert_ids.shape[1]
    ff = w_gate.shape[2]
    cap = count // GROUPS
    gs = width // GROUPS
    hbm = pl.BlockSpec(memory_space=pltpu.HBM)
    bf, f32 = jnp.bfloat16, jnp.float32
    dma = pltpu.SemaphoreType.DMA
    return pl.pallas_call(
        functools.partial(kernel, width, n_tp),
        out_shape=pltpu.VMEM((count, dmodel), bf),
        in_specs=[hbm] * 8,
        out_specs=pl.BlockSpec(memory_space=pltpu.VMEM),
        scratch_shapes=[
            pltpu.VMEM((count, dmodel), bf),
            pltpu.VMEM((1, dmodel), f32),
            pltpu.VMEM((1, count), f32),
            pltpu.VMEM((topk, count), f32),
            pltpu.VMEM((topk, count), jnp.int32),
            pltpu.VMEM((2, n_tp, dmodel, ff), bf),
            pltpu.VMEM((n_tp, ff, dmodel), bf),
            pltpu.VMEM((cap, dmodel), bf),
            pltpu.VMEM((cap, 128), f32),
            pltpu.VMEM((cap, 128), f32),
            pltpu.VMEM((gs, cap, dmodel), bf),
            pltpu.VMEM((gs, cap, dmodel), bf),
            pltpu.VMEM((gs, cap, dmodel), bf),
            pltpu.VMEM((cap, dmodel), bf),
            pltpu.VMEM((2, cap, dmodel), bf),
            pltpu.VMEM((n_tp, cap, dmodel), bf),
            dma((5,)), dma((3,)), dma((2,)), dma((2 * CHUNKS,)),
            dma, dma((CHUNKS,)), dma, dma,
            dma, dma((2, CHUNKS)), dma, dma((CHUNKS,)),
            dma, dma((CHUNKS,)), dma, dma((CHUNKS,)),
        ],
        compiler_params=pltpu.CompilerParams(collective_id=0, has_side_effects=True),
        name="expert_mixture",
    )(
        tokens, norm_gain.reshape(1, dmodel), group_prob.reshape(1, count), route_logits.T,
        expert_ids.T, w_gate, w_up, w_down,
    )


def solution(mesh):
    in_specs = (
        P(("grp", "ep"), None),
        P(),
        P(("grp", "ep")),
        P(("grp", "ep"), None),
        P(("grp", "ep"), None),
        P("ep", None, "tp"),
        P("ep", None, "tp"),
        P("ep", "tp", None),
    )
    out_specs = P(("grp", "ep"), None)
    return jax.shard_map(shards, mesh=mesh, in_specs=in_specs, out_specs=out_specs, check_vma=False)
```

```python
import functools

import jax
import jax.numpy as jnp
from jax import lax
from jax.experimental import pallas as pl
from jax.experimental.pallas import tpu as pltpu
from jax.sharding import PartitionSpec as P

GROUPS = 2
CHUNKS = 4
FIRST = 2
HOLD = 3
MESH = pl.DeviceIdType.MESH


def kernel(
    width, n_tp,
    tok_hbm, gain_hbm, prob_hbm, logit_hbm, ids_hbm, wg_hbm, wu_hbm, wd_hbm,
    out_ref,
    tok, gain, prob, logit, ids, wi, wd, send, wsend, wroot, x, outs, back, red, got, mixed,
    in_sem, wl_sem, ws_sem, wr_sem, xs_sem, xr_sem, vs_sem, vr_sem,
    ds_sem, dr_sem, bs_sem, br_sem, cs_sem, cr_sem, ms_sem, mr_sem, es_sem,
):
    e = lax.axis_index("ep")
    q = lax.axis_index("tp")
    sib = n_tp - 1 - q
    gs = width // GROUPS
    count, dmodel = tok.shape
    cap = count // GROUPS
    topk = ids.shape[0]
    block = e // gs
    local = e % gs
    base = block * gs
    partner = (e + gs) % width
    far = gs - 1 - local
    cross = q == n_tp - 1
    own = q != n_tp - 1
    group = (block + q) % GROUPS
    cw = dmodel // CHUNKS
    ff = wi.shape[3]
    f32, bf = jnp.float32, jnp.bfloat16
    split = cross & (block != 0)
    held = split & (local < 1)
    end = CHUNKS - 1

    def cols(c):
        return pl.ds(c * cw, cw)

    def peer(j):
        return base + (local + j) % gs

    def remote(src, dst, ss, rs, **where):
        return pltpu.make_async_remote_copy(
            src_ref=src, dst_ref=dst, send_sem=ss, recv_sem=rs,
            device_id=where, device_id_type=MESH,
        )

    smalls = [
        pltpu.make_async_copy(src, dst, in_sem.at[i])
        for i, (src, dst) in enumerate(
            [(tok_hbm, tok), (gain_hbm, gain), (prob_hbm, prob), (logit_hbm, logit), (ids_hbm, ids)]
        )
    ]
    for c in smalls:
        c.start()
    loads = [
        pltpu.make_async_copy(src.at[0], dst, wl_sem.at[i])
        for i, (src, dst) in enumerate([(wg_hbm, wi.at[0, q]), (wu_hbm, wi.at[1, q]), (wd_hbm, wd.at[q])])
    ]
    for c in loads:
        c.start()

    barrier = pltpu.get_barrier_semaphore()

    @pl.when(cross)
    def _():
        pl.semaphore_signal(barrier, inc=1, device_id={"ep": partner}, device_id_type=MESH)

    for j in range(1, gs):
        pl.semaphore_signal(barrier, inc=1, device_id={"ep": peer(j)}, device_id_type=MESH)
    pl.semaphore_signal(barrier, inc=1, device_id={"tp": sib}, device_id_type=MESH)

    for c in smalls:
        c.wait()
    values = tok[...].astype(f32)
    scale = lax.rsqrt(jnp.mean(values * values, axis=-1, keepdims=True) + 1e-06)
    normed = (values * scale * gain[...]).astype(bf)
    idv = ids[...]
    first = idv[0:1, :]
    grow = jnp.zeros((1, count), f32)
    for g in range(1, GROUPS):
        grow = grow + jnp.where(first >= g * gs, 1.0, 0.0)
    t_row = lax.broadcasted_iota(jnp.int32, (count, count), 0)
    t_col = lax.broadcasted_iota(jnp.int32, (count, count), 1)
    gfull = jnp.broadcast_to(grow, (count, count))
    gcol = jnp.sum(jnp.where(t_row == t_col, gfull, 0.0), axis=1, keepdims=True)
    same = jnp.where(gfull == gcol, 1.0, 0.0)
    pos_row = jnp.sum(jnp.where(t_row < t_col, same, 0.0), axis=0, keepdims=True)
    pos_col = jnp.sum(jnp.where(t_col < t_row, same, 0.0), axis=1, keepdims=True)
    r_io = lax.broadcasted_iota(jnp.int32, (cap, count), 0).astype(f32)
    place = jnp.where((pos_row == r_io) & (grow == group.astype(f32)), 1.0, 0.0)
    rows = jnp.dot(place.astype(bf), normed, preferred_element_type=f32).astype(bf)

    @pl.when(cross)
    def _():
        send[...] = rows

    @pl.when(own)
    def _():
        x[local] = rows

    pl.semaphore_wait(barrier, jnp.where(cross, gs + 1, gs))

    def across(c):
        return remote(send.at[:, cols(c)], x.at[local, :, cols(c)], xs_sem, xr_sem.at[c], ep=partner)

    def spread(j, c):
        part = x.at[local, :, cols(c)]
        return remote(part, part, ds_sem, dr_sem.at[jnp.where(split & (local >= FIRST), 1, 0), c], ep=peer(j))

    @pl.when(cross)
    def _():
        for c in range(CHUNKS):
            across(c).start()

    def spread_all():
        for c in range(CHUNKS):
            for j in range(1, gs):
                spread(j, c).start()

    @pl.when(own & (block == 0))
    def _():
        spread_all()

    def swap_in(h, c):
        part = wi.at[:, h, cols(c)]
        return remote(part, part, ws_sem.at[0], wr_sem.at[c], tp=sib)

    def swap_down(h, c):
        part = wd.at[h, :, cols(c)]
        return remote(part, part, ws_sem.at[1], wr_sem.at[CHUNKS + c], tp=sib)

    for c in loads[:2]:
        c.wait()
    for c in range(CHUNKS):
        swap_in(q, c).start()
    loads[2].wait()
    for c in range(CHUNKS):
        swap_down(q, c).start()

    expw = jnp.exp(logit[...])
    route = prob[...] * expw / jnp.sum(expw, axis=0, keepdims=True)
    k_io = lax.broadcasted_iota(jnp.int32, (128, count), 0)
    column = jnp.where(k_io < gs - 1, k_io + jnp.where(k_io >= far, 1, 0), far)
    column = jnp.where(k_io < gs, column, -1)
    within = idv - jnp.where(grow > 0.0, gs, 0)
    wtok = jnp.zeros((128, count), f32)
    for k in range(topk):
        wtok = wtok + jnp.where(within[k : k + 1, :] == column, route[k : k + 1, :], 0.0)

    def slots_of(placed):
        return lax.dot_general(
            placed, wtok, (((1,), (1,)), ((), ())),
            precision=lax.Precision.HIGHEST, preferred_element_type=f32,
        )

    def weights_across():
        return remote(wsend, wroot, vs_sem, vr_sem, ep=partner)

    there = jnp.where((pos_row == r_io) & (grow == (1 - block).astype(f32)), 1.0, 0.0)
    wsend[...] = slots_of(there)

    @pl.when(cross)
    def _():
        weights_across().start()

    @pl.when(own)
    def _():
        wroot[...] = slots_of(place)

    s_io = lax.broadcasted_iota(jnp.int32, (count, count), 1).astype(f32)
    role = jnp.where(gcol == block.astype(f32), 0.0, 1.0)
    unplace = jnp.where(s_io == role * cap + pos_col, 1.0, 0.0).astype(bf)

    late = own & (block != 0)

    @pl.when(late)
    def _():
        for c in range(HOLD):
            swap_in(sib, c).wait_recv()
        spread_all()

    @pl.when(cross)
    def _():
        for c in range(CHUNKS):
            across(c).wait_recv()
            for j in range(1, gs):
                spread(j, c).start()

    def landed(b, lo, hi, c):
        inside = (local >= lo) & (local < hi)

        def take(n):
            part = x.at[pl.ds(lo, n), :, cols(c)]
            remote(part, part, ds_sem, dr_sem.at[b, c], tp=sib).wait_recv()

        if hi - lo == gs:
            take(gs - 1)
            return
        if hi - lo > 1:

            @pl.when(inside)
            def _():
                take(hi - lo - 1)

        @pl.when(jnp.logical_not(inside))
        def _():
            take(hi - lo)

    def give(r, c):
        return remote(
            outs.at[r, :, cols(c)], back.at[local, :, cols(c)], bs_sem, br_sem.at[c], ep=base + r
        )

    def both(src, place, c, sem, to):
        dst = got.at[place, :, cols(c)]
        remote(src, dst, sem, cr_sem.at[c], ep=to).start()
        if c == end:
            remote(src, dst, es_sem, cr_sem.at[c], ep=to, tp=sib).start()

    def send_direct(r, c):
        both(outs.at[r, :, cols(c)], 1, c, bs_sem, (base + r + gs) % width)

    def experts(b, lo, hi):
        n = (hi - lo) * cap
        gates = [jnp.zeros((n, ff), f32)] * n_tp
        ups = [jnp.zeros((n, ff), f32)] * n_tp
        for c in range(CHUNKS):
            landed(b, lo, hi, c)
            if b == 0 and c >= HOLD:
                swap_in(sib, c).wait_recv()
            elif b == 0:

                @pl.when(jnp.logical_not(late))
                def _():
                    swap_in(sib, c).wait_recv()

            k = slice(c * cw, (c + 1) * cw)
            xc = x[lo:hi, :, k].reshape(n, cw)
            for h in range(n_tp):
                gates[h] = gates[h] + jnp.dot(xc, wi[0, h, k], preferred_element_type=f32)
                ups[h] = ups[h] + jnp.dot(xc, wi[1, h, k], preferred_element_type=f32)
        acts = [((g / (1.0 + jnp.exp(-g))) * u).astype(bf) for g, u in zip(gates, ups)]

        def down(c):
            if b == 0:
                swap_down(sib, c).wait_recv()
            k = slice(c * cw, (c + 1) * cw)
            total = jnp.dot(acts[0], wd[0, :, k], preferred_element_type=f32)
            for h in range(1, n_tp):
                total = total + jnp.dot(acts[h], wd[h, :, k], preferred_element_type=f32)
            return total.astype(bf).reshape(hi - lo, cap, cw)

        ready = down(0)
        for c in range(CHUNKS):
            k = slice(c * cw, (c + 1) * cw)
            outs[lo:hi, :, k] = ready
            if c + 1 < CHUNKS:
                ready = down(c + 1)
            for r in range(lo, hi):

                @pl.when(local == r)
                def _():
                    back[r, :, k] = outs[r, :, k]

                @pl.when((local != r) & (own | (far != r)))
                def _():
                    give(r, c).start()

                @pl.when(cross & (far == r) & jnp.logical_not(held))
                def _():
                    send_direct(r, c)

    @pl.when(split)
    def _():
        experts(0, 0, FIRST)
        experts(1, FIRST, gs)

    @pl.when(jnp.logical_not(split))
    def _():
        experts(0, 0, gs)

    def share(c):
        part = mixed.at[q, :, cols(c)]
        return remote(part, part, ms_sem, mr_sem.at[c], tp=sib)

    def shared(c):
        part = mixed.at[sib, :, cols(c)]
        return remote(part, part, ms_sem, mr_sem.at[c], tp=sib)

    @pl.when(cross)
    def _():
        weights_across().wait_recv()

    wv = wroot[...]
    near = [i + jnp.where(i >= far, 1, 0) for i in range(gs - 1)]
    for c in range(CHUNKS):
        k = slice(c * cw, (c + 1) * cw)

        def returned(n):
            part = back.at[pl.ds(0, n), :, cols(c)]
            remote(part, part, bs_sem, br_sem.at[c], tp=sib).wait_recv()

        @pl.when(cross)
        def _():
            returned(gs - 2)

        @pl.when(own)
        def _():
            returned(gs - 1)

        acc = wv[:, 0:1] * back[near[0], :, k].astype(f32)
        for i in range(1, gs - 1):
            acc = acc + wv[:, i : i + 1] * back[near[i], :, k].astype(f32)

        @pl.when(cross)
        def _():
            red[:, k] = acc.astype(bf)
            both(red.at[:, cols(c)], 0, c, cs_sem, partner)

        @pl.when(own)
        def _():
            last = wv[:, gs - 1 : gs] * back[far, :, k].astype(f32)
            mixed[0, :, k] = (acc + last).astype(bf)
            share(c).start()

    @pl.when(held)
    def _():
        for c in range(CHUNKS):
            send_direct(far, c)

    def arrived(c):
        k = slice(c * cw, (c + 1) * cw)
        part = got.at[:, :, cols(c)]
        remote(part, part, cs_sem, cr_sem.at[c], tp=sib).wait_recv()
        last = wsend[:, gs - 1 : gs] * got[1, :, k].astype(f32)
        mixed[n_tp - 1, :, k] = (got[0, :, k].astype(f32) + last).astype(bf)

    def restore(c):
        k = slice(c * cw, (c + 1) * cw)
        slots = mixed[:, :, k].reshape(count, cw)
        out_ref[:, k] = jnp.dot(unplace, slots, preferred_element_type=f32).astype(bf)

    @pl.when(cross)
    def _():
        for c in range(CHUNKS):
            arrived(c)
            if c < end:
                share(c).start()
            if c > 0:
                shared(c - 1).wait_recv()
                restore(c - 1)
        shared(end).wait_recv()
        restore(end)

    @pl.when(own)
    def _():
        for c in range(end):
            shared(c).wait_recv()
            restore(c)
        arrived(end)
        restore(end)

    @pl.when(cross)
    def _():
        weights_across().wait_send()
        remote(send, send, xs_sem, xr_sem.at[0], tp=sib).wait_send()
        remote(red, red, cs_sem, cr_sem.at[0], tp=sib).wait_send()
        twice = got.at[:, :, cols(end)]
        remote(twice, twice, es_sem, cr_sem.at[0], tp=sib).wait_send()
        most_mixed = mixed.at[q, :, pl.ds(0, end * cw)]
        remote(most_mixed, most_mixed, ms_sem, mr_sem.at[0], tp=sib).wait_send()

    @pl.when(own)
    def _():
        remote(mixed.at[q], mixed.at[q], ms_sem, mr_sem.at[0], tp=sib).wait_send()

    half_in, half_down = wi.at[:, q], wd.at[q]
    remote(half_in, half_in, ws_sem.at[0], wr_sem.at[0], tp=sib).wait_send()
    remote(half_down, half_down, ws_sem.at[1], wr_sem.at[0], tp=sib).wait_send()
    most = x.at[pl.ds(0, gs - 1)]
    remote(most, most, ds_sem, dr_sem.at[0, 0], tp=sib).wait_send()
    remote(most, most, bs_sem, br_sem.at[0], tp=sib).wait_send()


def shards(tokens, norm_gain, group_prob, route_logits, expert_ids, w_gate, w_up, w_down):
    width = lax.axis_size("ep")
    n_tp = lax.axis_size("tp")
    count, dmodel = tokens.shape
    topk = expert_ids.shape[1]
    ff = w_gate.shape[2]
    cap = count // GROUPS
    gs = width // GROUPS
    hbm = pl.BlockSpec(memory_space=pltpu.HBM)
    bf, f32 = jnp.bfloat16, jnp.float32
    dma = pltpu.SemaphoreType.DMA
    return pl.pallas_call(
        functools.partial(kernel, width, n_tp),
        out_shape=pltpu.VMEM((count, dmodel), bf),
        in_specs=[hbm] * 8,
        out_specs=pl.BlockSpec(memory_space=pltpu.VMEM),
        scratch_shapes=[
            pltpu.VMEM((count, dmodel), bf),
            pltpu.VMEM((1, dmodel), f32),
            pltpu.VMEM((1, count), f32),
            pltpu.VMEM((topk, count), f32),
            pltpu.VMEM((topk, count), jnp.int32),
            pltpu.VMEM((2, n_tp, dmodel, ff), bf),
            pltpu.VMEM((n_tp, ff, dmodel), bf),
            pltpu.VMEM((cap, dmodel), bf),
            pltpu.VMEM((cap, 128), f32),
            pltpu.VMEM((cap, 128), f32),
            pltpu.VMEM((gs, cap, dmodel), bf),
            pltpu.VMEM((gs, cap, dmodel), bf),
            pltpu.VMEM((gs, cap, dmodel), bf),
            pltpu.VMEM((cap, dmodel), bf),
            pltpu.VMEM((2, cap, dmodel), bf),
            pltpu.VMEM((n_tp, cap, dmodel), bf),
            dma((5,)), dma((3,)), dma((2,)), dma((2 * CHUNKS,)),
            dma, dma((CHUNKS,)), dma, dma,
            dma, dma((2, CHUNKS)), dma, dma((CHUNKS,)),
            dma, dma((CHUNKS,)), dma, dma((CHUNKS,)), dma,
        ],
        compiler_params=pltpu.CompilerParams(collective_id=0, has_side_effects=True),
        name="expert_mixture",
    )(
        tokens, norm_gain.reshape(1, dmodel), group_prob.reshape(1, count), route_logits.T,
        expert_ids.T, w_gate, w_up, w_down,
    )


def solution(mesh):
    in_specs = (
        P(("grp", "ep"), None),
        P(),
        P(("grp", "ep")),
        P(("grp", "ep"), None),
        P(("grp", "ep"), None),
        P("ep", None, "tp"),
        P("ep", None, "tp"),
        P("ep", "tp", None),
    )
    out_specs = P(("grp", "ep"), None)
    return jax.shard_map(shards, mesh=mesh, in_specs=in_specs, out_specs=out_specs, check_vma=False)
```

```python
import functools

import jax
import jax.numpy as jnp
from jax import lax
from jax.experimental import pallas as pl
from jax.experimental.pallas import tpu as pltpu
from jax.sharding import PartitionSpec as P

GROUPS = 2
CHUNKS = 4
FIRST = 2
HOLD = 3
MESH = pl.DeviceIdType.MESH


def kernel(
    width, n_tp,
    tok_hbm, gain_hbm, prob_hbm, logit_hbm, ids_hbm, wg_hbm, wu_hbm, wd_hbm,
    out_ref,
    tok, gain, prob, logit, ids, wi, wd, send, wsend, wroot, x, outs, back, red, got, mixed,
    in_sem, wl_sem, out_sem, wr_sem, xr_sem, vr_sem, dr_sem, br_sem, cr_sem, mr_sem,
):
    e = lax.axis_index("ep")
    q = lax.axis_index("tp")
    sib = n_tp - 1 - q
    gs = width // GROUPS
    count, dmodel = tok.shape
    cap = count // GROUPS
    topk = ids.shape[0]
    block = e // gs
    local = e % gs
    base = block * gs
    partner = (e + gs) % width
    far = gs - 1 - local
    cross = q == n_tp - 1
    own = q != n_tp - 1
    group = (block + q) % GROUPS
    cw = dmodel // CHUNKS
    ff = wi.shape[3]
    f32, bf = jnp.float32, jnp.bfloat16
    split = cross & (block != 0)
    held = split & (local < 1)
    end = CHUNKS - 1

    def cols(c):
        return pl.ds(c * cw, cw)

    def peer(j):
        return base + (local + j) % gs

    def remote(src, dst, ss, rs, **where):
        return pltpu.make_async_remote_copy(
            src_ref=src, dst_ref=dst, send_sem=ss, recv_sem=rs,
            device_id=where, device_id_type=MESH,
        )

    smalls = [
        pltpu.make_async_copy(src, dst, in_sem)
        for src, dst in [
            (tok_hbm, tok), (gain_hbm, gain), (prob_hbm, prob), (logit_hbm, logit), (ids_hbm, ids)
        ]
    ]
    for c in smalls:
        c.start()
    loads = [
        pltpu.make_async_copy(src.at[0], dst, wl_sem.at[i // 2])
        for i, (src, dst) in enumerate([(wg_hbm, wi.at[0, q]), (wu_hbm, wi.at[1, q]), (wd_hbm, wd.at[q])])
    ]
    for c in loads:
        c.start()

    barrier = pltpu.get_barrier_semaphore()

    @pl.when(cross)
    def _():
        pl.semaphore_signal(barrier, inc=1, device_id={"ep": partner}, device_id_type=MESH)

    for j in range(1, gs):
        pl.semaphore_signal(barrier, inc=1, device_id={"ep": peer(j)}, device_id_type=MESH)
    pl.semaphore_signal(barrier, inc=1, device_id={"tp": sib}, device_id_type=MESH)

    for c in smalls:
        c.wait()
    values = tok[...].astype(f32)
    scale = lax.rsqrt(jnp.mean(values * values, axis=-1, keepdims=True) + 1e-06)
    normed = (values * scale * gain[...]).astype(bf)
    idv = ids[...]
    first = idv[0:1, :]
    grow = jnp.zeros((1, count), f32)
    for g in range(1, GROUPS):
        grow = grow + jnp.where(first >= g * gs, 1.0, 0.0)
    t_row = lax.broadcasted_iota(jnp.int32, (count, count), 0)
    t_col = lax.broadcasted_iota(jnp.int32, (count, count), 1)
    gfull = jnp.broadcast_to(grow, (count, count))
    gcol = jnp.sum(jnp.where(t_row == t_col, gfull, 0.0), axis=1, keepdims=True)
    same = jnp.where(gfull == gcol, 1.0, 0.0)
    pos_row = jnp.sum(jnp.where(t_row < t_col, same, 0.0), axis=0, keepdims=True)
    pos_col = jnp.sum(jnp.where(t_col < t_row, same, 0.0), axis=1, keepdims=True)
    r_io = lax.broadcasted_iota(jnp.int32, (cap, count), 0).astype(f32)
    place = jnp.where((pos_row == r_io) & (grow == group.astype(f32)), 1.0, 0.0)
    rows = jnp.dot(place.astype(bf), normed, preferred_element_type=f32).astype(bf)

    @pl.when(cross)
    def _():
        send[...] = rows

    @pl.when(own)
    def _():
        x[local] = rows

    pl.semaphore_wait(barrier, jnp.where(cross, gs + 1, gs))

    def across(c):
        return remote(send.at[:, cols(c)], x.at[local, :, cols(c)], out_sem, xr_sem.at[c], ep=partner)

    def spread(j, c):
        part = x.at[local, :, cols(c)]
        return remote(part, part, out_sem, dr_sem.at[jnp.where(split & (local >= FIRST), CHUNKS, c)], ep=peer(j))

    @pl.when(cross)
    def _():
        for c in range(CHUNKS):
            across(c).start()

    def spread_all():
        for c in range(CHUNKS):
            for j in range(1, gs):
                spread(j, c).start()

    @pl.when(own & (block == 0))
    def _():
        spread_all()

    def swap_in(h, c):
        part = wi.at[:, h, cols(c)]
        return remote(part, part, out_sem, wr_sem.at[c], tp=sib)

    def swap_down(h, c):
        part = wd.at[h, :, cols(c)]
        return remote(part, part, out_sem, wr_sem.at[CHUNKS + c], tp=sib)

    for c in loads[:2]:
        c.wait()
    for c in range(CHUNKS):
        swap_in(q, c).start()
    loads[2].wait()
    for c in range(CHUNKS):
        swap_down(q, c).start()

    expw = jnp.exp(logit[...])
    route = prob[...] * expw / jnp.sum(expw, axis=0, keepdims=True)
    k_io = lax.broadcasted_iota(jnp.int32, (128, count), 0)
    column = jnp.where(k_io < gs - 1, k_io + jnp.where(k_io >= far, 1, 0), far)
    column = jnp.where(k_io < gs, column, -1)
    within = idv - jnp.where(grow > 0.0, gs, 0)
    wtok = jnp.zeros((128, count), f32)
    for k in range(topk):
        wtok = wtok + jnp.where(within[k : k + 1, :] == column, route[k : k + 1, :], 0.0)

    def slots_of(placed):
        return lax.dot_general(
            placed, wtok, (((1,), (1,)), ((), ())),
            precision=lax.Precision.HIGHEST, preferred_element_type=f32,
        )

    def weights_across():
        return remote(wsend, wroot, out_sem, vr_sem, ep=partner)

    there = jnp.where((pos_row == r_io) & (grow == (1 - block).astype(f32)), 1.0, 0.0)
    wsend[...] = slots_of(there)

    @pl.when(cross)
    def _():
        weights_across().start()

    @pl.when(own)
    def _():
        wroot[...] = slots_of(place)

    s_io = lax.broadcasted_iota(jnp.int32, (count, count), 1).astype(f32)
    role = jnp.where(gcol == block.astype(f32), 0.0, 1.0)
    unplace = jnp.where(s_io == role * cap + pos_col, 1.0, 0.0).astype(bf)

    late = own & (block != 0)

    @pl.when(late)
    def _():
        for c in range(HOLD):
            swap_in(sib, c).wait_recv()
        spread_all()

    @pl.when(cross)
    def _():
        for c in range(CHUNKS):
            across(c).wait_recv()
            for j in range(1, gs):
                spread(j, c).start()

    def landed(b, lo, hi, c):
        inside = (local >= lo) & (local < hi)

        def take(n):
            part = x.at[pl.ds(lo, n), :, cols(c)] if b == 0 else x.at[pl.ds(lo, n)]
            sem = dr_sem.at[c if b == 0 else CHUNKS]
            remote(part, part, out_sem, sem, tp=sib).wait_recv()

        if b > 0 and c > 0:
            return
        if hi - lo == gs:
            take(gs - 1)
            return
        if hi - lo > 1:

            @pl.when(inside)
            def _():
                take(hi - lo - 1)

        @pl.when(jnp.logical_not(inside))
        def _():
            take(hi - lo)

    def give(r, c):
        return remote(
            outs.at[r, :, cols(c)], back.at[local, :, cols(c)], out_sem, br_sem.at[c], ep=base + r
        )

    def both(src, place, c, sem, to):
        dst = got.at[place, :, cols(c)]
        remote(src, dst, sem, cr_sem.at[c], ep=to).start()
        if c == end:
            remote(src, dst, out_sem, cr_sem.at[c], ep=to, tp=sib).start()

    def send_direct(r, c):
        both(outs.at[r, :, cols(c)], 1, c, out_sem, (base + r + gs) % width)

    def experts(b, lo, hi):
        n = (hi - lo) * cap
        gates = [jnp.zeros((n, ff), f32)] * n_tp
        ups = [jnp.zeros((n, ff), f32)] * n_tp
        for c in range(CHUNKS):
            landed(b, lo, hi, c)
            if b == 0 and c >= HOLD:
                swap_in(sib, c).wait_recv()
            elif b == 0:

                @pl.when(jnp.logical_not(late))
                def _():
                    swap_in(sib, c).wait_recv()

            k = slice(c * cw, (c + 1) * cw)
            xc = x[lo:hi, :, k].reshape(n, cw)
            for h in range(n_tp):
                gates[h] = gates[h] + jnp.dot(xc, wi[0, h, k], preferred_element_type=f32)
                ups[h] = ups[h] + jnp.dot(xc, wi[1, h, k], preferred_element_type=f32)
        acts = [((g / (1.0 + jnp.exp(-g))) * u).astype(bf) for g, u in zip(gates, ups)]

        def down(c):
            if b == 0:
                swap_down(sib, c).wait_recv()
            k = slice(c * cw, (c + 1) * cw)
            total = jnp.dot(acts[0], wd[0, :, k], preferred_element_type=f32)
            for h in range(1, n_tp):
                total = total + jnp.dot(acts[h], wd[h, :, k], preferred_element_type=f32)
            return total.astype(bf).reshape(hi - lo, cap, cw)

        ready = down(0)
        for c in range(CHUNKS):
            k = slice(c * cw, (c + 1) * cw)
            outs[lo:hi, :, k] = ready
            if c + 1 < CHUNKS:
                ready = down(c + 1)
            for r in range(lo, hi):

                @pl.when(local == r)
                def _():
                    back[r, :, k] = outs[r, :, k]

                @pl.when((local != r) & (own | (far != r)))
                def _():
                    give(r, c).start()

                @pl.when(cross & (far == r) & jnp.logical_not(held))
                def _():
                    send_direct(r, c)

    @pl.when(split)
    def _():
        experts(0, 0, FIRST)
        experts(1, FIRST, gs)

    @pl.when(jnp.logical_not(split))
    def _():
        experts(0, 0, gs)

    def share(c):
        part = mixed.at[q, :, cols(c)]
        return remote(part, part, out_sem, mr_sem.at[c], tp=sib)

    def shared(c):
        part = mixed.at[sib, :, cols(c)]
        return remote(part, part, out_sem, mr_sem.at[c], tp=sib)

    @pl.when(cross)
    def _():
        weights_across().wait_recv()

    wv = wroot[...]
    near = [i + jnp.where(i >= far, 1, 0) for i in range(gs - 1)]
    for c in range(CHUNKS):
        k = slice(c * cw, (c + 1) * cw)

        def returned(n):
            part = back.at[pl.ds(0, n), :, cols(c)]
            remote(part, part, out_sem, br_sem.at[c], tp=sib).wait_recv()

        @pl.when(cross)
        def _():
            returned(gs - 2)

        @pl.when(own)
        def _():
            returned(gs - 1)

        acc = wv[:, 0:1] * back[near[0], :, k].astype(f32)
        for i in range(1, gs - 1):
            acc = acc + wv[:, i : i + 1] * back[near[i], :, k].astype(f32)

        @pl.when(cross)
        def _():
            red[:, k] = acc.astype(bf)
            both(red.at[:, cols(c)], 0, c, out_sem, partner)

        @pl.when(own)
        def _():
            last = wv[:, gs - 1 : gs] * back[far, :, k].astype(f32)
            mixed[0, :, k] = (acc + last).astype(bf)
            share(c).start()

    @pl.when(held)
    def _():
        for c in range(CHUNKS):
            send_direct(far, c)

    def arrived(c):
        k = slice(c * cw, (c + 1) * cw)
        part = got.at[:, :, cols(c)]
        remote(part, part, out_sem, cr_sem.at[c], tp=sib).wait_recv()
        last = wsend[:, gs - 1 : gs] * got[1, :, k].astype(f32)
        mixed[n_tp - 1, :, k] = (got[0, :, k].astype(f32) + last).astype(bf)

    def restore(c):
        k = slice(c * cw, (c + 1) * cw)
        slots = mixed[:, :, k].reshape(count, cw)
        out_ref[:, k] = jnp.dot(unplace, slots, preferred_element_type=f32).astype(bf)

    @pl.when(cross)
    def _():
        for c in range(CHUNKS):
            arrived(c)
            if c < end:
                share(c).start()
            if c > 0:
                shared(c - 1).wait_recv()
                restore(c - 1)
        shared(end).wait_recv()
        restore(end)

    @pl.when(own)
    def _():
        for c in range(end):
            shared(c).wait_recv()
            restore(c)
        arrived(end)
        restore(end)

    @pl.when(cross)
    def _():
        weights_across().wait_send()
        remote(send, send, out_sem, xr_sem.at[0], tp=sib).wait_send()
        remote(red, red, out_sem, cr_sem.at[0], tp=sib).wait_send()
        twice = got.at[:, :, cols(end)]
        remote(twice, twice, out_sem, cr_sem.at[0], tp=sib).wait_send()
        most_mixed = mixed.at[q, :, pl.ds(0, end * cw)]
        remote(most_mixed, most_mixed, out_sem, mr_sem.at[0], tp=sib).wait_send()

    @pl.when(own)
    def _():
        remote(mixed.at[q], mixed.at[q], out_sem, mr_sem.at[0], tp=sib).wait_send()

    half_in, half_down = wi.at[:, q], wd.at[q]
    remote(half_in, half_in, out_sem, wr_sem.at[0], tp=sib).wait_send()
    remote(half_down, half_down, out_sem, wr_sem.at[0], tp=sib).wait_send()
    most = x.at[pl.ds(0, gs - 1)]
    remote(most, most, out_sem, dr_sem.at[0], tp=sib).wait_send()
    remote(most, most, out_sem, br_sem.at[0], tp=sib).wait_send()


def shards(tokens, norm_gain, group_prob, route_logits, expert_ids, w_gate, w_up, w_down):
    width = lax.axis_size("ep")
    n_tp = lax.axis_size("tp")
    count, dmodel = tokens.shape
    topk = expert_ids.shape[1]
    ff = w_gate.shape[2]
    cap = count // GROUPS
    gs = width // GROUPS
    hbm = pl.BlockSpec(memory_space=pltpu.HBM)
    bf, f32 = jnp.bfloat16, jnp.float32
    dma = pltpu.SemaphoreType.DMA
    return pl.pallas_call(
        functools.partial(kernel, width, n_tp),
        out_shape=pltpu.VMEM((count, dmodel), bf),
        in_specs=[hbm] * 8,
        out_specs=pl.BlockSpec(memory_space=pltpu.VMEM),
        scratch_shapes=[
            pltpu.VMEM((count, dmodel), bf),
            pltpu.VMEM((1, dmodel), f32),
            pltpu.VMEM((1, count), f32),
            pltpu.VMEM((topk, count), f32),
            pltpu.VMEM((topk, count), jnp.int32),
            pltpu.VMEM((2, n_tp, dmodel, ff), bf),
            pltpu.VMEM((n_tp, ff, dmodel), bf),
            pltpu.VMEM((cap, dmodel), bf),
            pltpu.VMEM((cap, 128), f32),
            pltpu.VMEM((cap, 128), f32),
            pltpu.VMEM((gs, cap, dmodel), bf),
            pltpu.VMEM((gs, cap, dmodel), bf),
            pltpu.VMEM((gs, cap, dmodel), bf),
            pltpu.VMEM((cap, dmodel), bf),
            pltpu.VMEM((2, cap, dmodel), bf),
            pltpu.VMEM((n_tp, cap, dmodel), bf),
            dma, dma((2,)), dma, dma((2 * CHUNKS,)), dma((CHUNKS,)), dma,
            dma((CHUNKS + 1,)), dma((CHUNKS,)), dma((CHUNKS,)), dma((CHUNKS,)),
        ],
        compiler_params=pltpu.CompilerParams(collective_id=0, has_side_effects=True),
        name="expert_mixture",
    )(
        tokens, norm_gain.reshape(1, dmodel), group_prob.reshape(1, count), route_logits.T,
        expert_ids.T, w_gate, w_up, w_down,
    )


def solution(mesh):
    in_specs = (
        P(("grp", "ep"), None),
        P(),
        P(("grp", "ep")),
        P(("grp", "ep"), None),
        P(("grp", "ep"), None),
        P("ep", None, "tp"),
        P("ep", None, "tp"),
        P("ep", "tp", None),
    )
    out_specs = P(("grp", "ep"), None)
    return jax.shard_map(shards, mesh=mesh, in_specs=in_specs, out_specs=out_specs, check_vma=False)
```

```python
import functools

import jax
import jax.numpy as jnp
from jax import lax
from jax.experimental import pallas as pl
from jax.experimental.pallas import tpu as pltpu
from jax.sharding import PartitionSpec as P

GROUPS = 2
CHUNKS = 4
FIRST = 2
HOLD = 3
TWICE = 1
MESH = pl.DeviceIdType.MESH


def kernel(
    width, n_tp,
    tok_hbm, gain_hbm, prob_hbm, logit_hbm, ids_hbm, wg_hbm, wu_hbm, wd_hbm,
    out_ref,
    tok, gain, prob, logit, ids, wi, wd, send, wsend, wroot, x, outs, back, red, got, mixed,
    in_sem, wl_sem, out_sem, wr_sem, xr_sem, vr_sem, dr_sem, br_sem, cr_sem, mr_sem,
):
    e = lax.axis_index("ep")
    q = lax.axis_index("tp")
    sib = n_tp - 1 - q
    gs = width // GROUPS
    count, dmodel = tok.shape
    cap = count // GROUPS
    topk = ids.shape[0]
    block = e // gs
    local = e % gs
    base = block * gs
    partner = (e + gs) % width
    far = gs - 1 - local
    cross = q == n_tp - 1
    own = q != n_tp - 1
    group = (block + q) % GROUPS
    cw = dmodel // CHUNKS
    ff = wi.shape[3]
    f32, bf = jnp.float32, jnp.bfloat16
    split = cross & (block != 0)
    held = split & (local < 1)
    end = CHUNKS - TWICE

    def cols(c):
        return pl.ds(c * cw, cw)

    def peer(j):
        return base + (local + j) % gs

    def remote(src, dst, ss, rs, **where):
        return pltpu.make_async_remote_copy(
            src_ref=src, dst_ref=dst, send_sem=ss, recv_sem=rs,
            device_id=where, device_id_type=MESH,
        )

    smalls = [
        pltpu.make_async_copy(src, dst, in_sem)
        for src, dst in [
            (tok_hbm, tok), (gain_hbm, gain), (prob_hbm, prob), (logit_hbm, logit), (ids_hbm, ids)
        ]
    ]
    for c in smalls:
        c.start()
    loads = [
        pltpu.make_async_copy(src.at[0], dst, wl_sem.at[i // 2])
        for i, (src, dst) in enumerate([(wg_hbm, wi.at[0, q]), (wu_hbm, wi.at[1, q]), (wd_hbm, wd.at[q])])
    ]
    for c in loads:
        c.start()

    barrier = pltpu.get_barrier_semaphore()

    @pl.when(cross)
    def _():
        pl.semaphore_signal(barrier, inc=1, device_id={"ep": partner}, device_id_type=MESH)

    for j in range(1, gs):
        pl.semaphore_signal(barrier, inc=1, device_id={"ep": peer(j)}, device_id_type=MESH)
    pl.semaphore_signal(barrier, inc=1, device_id={"tp": sib}, device_id_type=MESH)

    for c in smalls:
        c.wait()
    values = tok[...].astype(f32)
    scale = lax.rsqrt(jnp.mean(values * values, axis=-1, keepdims=True) + 1e-06)
    normed = (values * scale * gain[...]).astype(bf)
    idv = ids[...]
    first = idv[0:1, :]
    grow = jnp.zeros((1, count), f32)
    for g in range(1, GROUPS):
        grow = grow + jnp.where(first >= g * gs, 1.0, 0.0)
    t_row = lax.broadcasted_iota(jnp.int32, (count, count), 0)
    t_col = lax.broadcasted_iota(jnp.int32, (count, count), 1)
    gfull = jnp.broadcast_to(grow, (count, count))
    gcol = jnp.sum(jnp.where(t_row == t_col, gfull, 0.0), axis=1, keepdims=True)
    same = jnp.where(gfull == gcol, 1.0, 0.0)
    pos_row = jnp.sum(jnp.where(t_row < t_col, same, 0.0), axis=0, keepdims=True)
    pos_col = jnp.sum(jnp.where(t_col < t_row, same, 0.0), axis=1, keepdims=True)
    r_io = lax.broadcasted_iota(jnp.int32, (cap, count), 0).astype(f32)
    place = jnp.where((pos_row == r_io) & (grow == group.astype(f32)), 1.0, 0.0)
    rows = jnp.dot(place.astype(bf), normed, preferred_element_type=f32).astype(bf)

    @pl.when(cross)
    def _():
        send[...] = rows

    @pl.when(own)
    def _():
        x[local] = rows

    pl.semaphore_wait(barrier, jnp.where(cross, gs + 1, gs))

    def across(c):
        return remote(send.at[:, cols(c)], x.at[local, :, cols(c)], out_sem, xr_sem.at[c], ep=partner)

    def spread(j, c):
        part = x.at[local, :, cols(c)]
        return remote(part, part, out_sem, dr_sem.at[jnp.where(split & (local >= FIRST), CHUNKS, c)], ep=peer(j))

    @pl.when(cross)
    def _():
        for c in range(CHUNKS):
            across(c).start()

    def spread_all():
        for c in range(CHUNKS):
            for j in [*range(1, gs, 2), *range(2, gs, 2)]:
                spread(j, c).start()

    @pl.when(own & (block == 0))
    def _():
        spread_all()

    def swap_in(h, c):
        part = wi.at[:, h, cols(c)]
        return remote(part, part, out_sem, wr_sem.at[c], tp=sib)

    def swap_down(h, c):
        part = wd.at[h, :, cols(c)]
        return remote(part, part, out_sem, wr_sem.at[CHUNKS + c], tp=sib)

    for c in loads[:2]:
        c.wait()
    for c in range(CHUNKS):
        swap_in(q, c).start()
    loads[2].wait()
    for c in range(CHUNKS):
        swap_down(q, c).start()

    expw = jnp.exp(logit[...])
    route = prob[...] * expw / jnp.sum(expw, axis=0, keepdims=True)
    k_io = lax.broadcasted_iota(jnp.int32, (128, count), 0)
    column = jnp.where(k_io < gs - 1, k_io + jnp.where(k_io >= far, 1, 0), far)
    column = jnp.where(k_io < gs, column, -1)
    within = idv - jnp.where(grow > 0.0, gs, 0)
    wtok = jnp.zeros((128, count), f32)
    for k in range(topk):
        wtok = wtok + jnp.where(within[k : k + 1, :] == column, route[k : k + 1, :], 0.0)

    def slots_of(placed):
        return lax.dot_general(
            placed, wtok, (((1,), (1,)), ((), ())),
            precision=lax.Precision.HIGHEST, preferred_element_type=f32,
        )

    def weights_across():
        return remote(wsend, wroot, out_sem, vr_sem, ep=partner)

    there = jnp.where((pos_row == r_io) & (grow == (1 - block).astype(f32)), 1.0, 0.0)
    wsend[...] = slots_of(there)

    @pl.when(cross)
    def _():
        weights_across().start()

    @pl.when(own)
    def _():
        wroot[...] = slots_of(place)

    s_io = lax.broadcasted_iota(jnp.int32, (count, count), 1).astype(f32)
    role = jnp.where(gcol == block.astype(f32), 0.0, 1.0)
    unplace = jnp.where(s_io == role * cap + pos_col, 1.0, 0.0).astype(bf)

    late = own & (block != 0)

    @pl.when(late)
    def _():
        for c in range(HOLD):
            swap_in(sib, c).wait_recv()
        spread_all()

    @pl.when(cross)
    def _():
        for c in range(CHUNKS):
            across(c).wait_recv()
            for j in [*range(1, gs, 2), *range(2, gs, 2)]:
                spread(j, c).start()

    def landed(b, lo, hi, c):
        inside = (local >= lo) & (local < hi)

        def take(n):
            part = x.at[pl.ds(lo, n), :, cols(c)] if b == 0 else x.at[pl.ds(lo, n)]
            sem = dr_sem.at[c if b == 0 else CHUNKS]
            remote(part, part, out_sem, sem, tp=sib).wait_recv()

        if b > 0 and c > 0:
            return
        if hi - lo == gs:
            take(gs - 1)
            return
        if hi - lo > 1:

            @pl.when(inside)
            def _():
                take(hi - lo - 1)

        @pl.when(jnp.logical_not(inside))
        def _():
            take(hi - lo)

    def give(r, c):
        return remote(
            outs.at[r, :, cols(c)], back.at[local, :, cols(c)], out_sem, br_sem.at[c], ep=base + r
        )

    def both(src, place, c, sem, to):
        dst = got.at[place, :, cols(c)]
        early = place == 1 and c == end
        remote(src, dst, sem, cr_sem.at[CHUNKS if early else c], ep=to).start()
        if c >= end and place == 0:
            remote(src, dst, out_sem, cr_sem.at[c], ep=to, tp=sib).start()

    def send_direct(r, c):
        both(outs.at[r, :, cols(c)], 1, c, out_sem, (base + r + gs) % width)

    def experts(b, lo, hi):
        n = (hi - lo) * cap
        gates = [jnp.zeros((n, ff), f32)] * n_tp
        ups = [jnp.zeros((n, ff), f32)] * n_tp
        for c in range(CHUNKS):
            landed(b, lo, hi, c)
            if b == 0 and c >= HOLD:
                swap_in(sib, c).wait_recv()
            elif b == 0:

                @pl.when(jnp.logical_not(late))
                def _():
                    swap_in(sib, c).wait_recv()

            k = slice(c * cw, (c + 1) * cw)
            xc = x[lo:hi, :, k].reshape(n, cw)
            for h in range(n_tp):
                gates[h] = gates[h] + jnp.dot(xc, wi[0, h, k], preferred_element_type=f32)
                ups[h] = ups[h] + jnp.dot(xc, wi[1, h, k], preferred_element_type=f32)
        acts = [((g / (1.0 + jnp.exp(-g))) * u).astype(bf) for g, u in zip(gates, ups)]

        def down(c):
            if b == 0:
                swap_down(sib, c).wait_recv()
            k = slice(c * cw, (c + 1) * cw)
            total = jnp.dot(acts[0], wd[0, :, k], preferred_element_type=f32)
            for h in range(1, n_tp):
                total = total + jnp.dot(acts[h], wd[h, :, k], preferred_element_type=f32)
            return total.astype(bf).reshape(hi - lo, cap, cw)

        ready = down(0)
        for c in range(CHUNKS):
            k = slice(c * cw, (c + 1) * cw)
            outs[lo:hi, :, k] = ready
            if c + 1 < CHUNKS:
                ready = down(c + 1)
            for r in range(lo, hi):

                @pl.when(local == r)
                def _():
                    back[r, :, k] = outs[r, :, k]

                @pl.when((local != r) & (own | (far != r)))
                def _():
                    give(r, c).start()

                @pl.when(cross & (far == r) & jnp.logical_not(held))
                def _():
                    send_direct(r, c)

    @pl.when(split)
    def _():
        experts(0, 0, FIRST)
        experts(1, FIRST, gs)

    @pl.when(jnp.logical_not(split))
    def _():
        experts(0, 0, gs)

    def share(c):
        part = mixed.at[q, :, cols(c)]
        return remote(part, part, out_sem, mr_sem.at[c], tp=sib)

    def shared(c):
        part = mixed.at[sib, :, cols(c)]
        return remote(part, part, out_sem, mr_sem.at[c], tp=sib)

    @pl.when(cross)
    def _():
        weights_across().wait_recv()

    wv = wroot[...]
    near = [i + jnp.where(i >= far, 1, 0) for i in range(gs - 1)]
    for c in range(CHUNKS):
        k = slice(c * cw, (c + 1) * cw)

        def returned(n):
            part = back.at[pl.ds(0, n), :, cols(c)]
            remote(part, part, out_sem, br_sem.at[c], tp=sib).wait_recv()

        @pl.when(cross)
        def _():
            returned(gs - 2)

        @pl.when(own)
        def _():
            returned(gs - 1)

        acc = wv[:, 0:1] * back[near[0], :, k].astype(f32)
        for i in range(1, gs - 1):
            acc = acc + wv[:, i : i + 1] * back[near[i], :, k].astype(f32)

        @pl.when(cross)
        def _():
            red[:, k] = acc.astype(bf)
            both(red.at[:, cols(c)], 0, c, out_sem, partner)

        @pl.when(own)
        def _():
            last = wv[:, gs - 1 : gs] * back[far, :, k].astype(f32)
            mixed[0, :, k] = (acc + last).astype(bf)
            share(c).start()

    @pl.when(held)
    def _():
        for c in range(CHUNKS):
            send_direct(far, c)

    spot = got.at[1, :, cols(end)]

    def pass_on():
        return remote(spot, spot, out_sem, cr_sem.at[CHUNKS], tp=sib)

    def arrived(c):
        k = slice(c * cw, (c + 1) * cw)
        part = got.at[0, :, cols(c)] if c == end else got.at[:, :, cols(c)]
        remote(part, part, out_sem, cr_sem.at[c], tp=sib).wait_recv()
        last = wsend[:, gs - 1 : gs] * got[1, :, k].astype(f32)
        mixed[n_tp - 1, :, k] = (got[0, :, k].astype(f32) + last).astype(bf)

    def restore(c):
        k = slice(c * cw, (c + 1) * cw)
        slots = mixed[:, :, k].reshape(count, cw)
        out_ref[:, k] = jnp.dot(unplace, slots, preferred_element_type=f32).astype(bf)

    @pl.when(cross)
    def _():
        pass_on().wait_recv()
        pass_on().start()
        for c in range(CHUNKS):
            arrived(c)
            if c < end:
                share(c).start()
            if c == end - 1:
                for d in range(c):
                    shared(d).wait_recv()
                    restore(d)
            if c >= end:
                shared(c - 1).wait_recv()
                restore(c - 1)
        shared(CHUNKS - 1).wait_recv()
        restore(CHUNKS - 1)

    @pl.when(own)
    def _():
        for c in range(end):
            shared(c).wait_recv()
            restore(c)
        pass_on().wait_recv()
        arrived(end)
        restore(end)

    @pl.when(cross)
    def _():
        weights_across().wait_send()
        remote(send, send, out_sem, xr_sem.at[0], tp=sib).wait_send()
        remote(red, red, out_sem, cr_sem.at[0], tp=sib).wait_send()
        twice = got.at[:, :, pl.ds(end * cw, TWICE * cw)]
        remote(twice, twice, out_sem, cr_sem.at[0], tp=sib).wait_send()
        most_mixed = mixed.at[q, :, pl.ds(0, end * cw)]
        remote(most_mixed, most_mixed, out_sem, mr_sem.at[0], tp=sib).wait_send()

    @pl.when(own)
    def _():
        remote(mixed.at[q], mixed.at[q], out_sem, mr_sem.at[0], tp=sib).wait_send()

    half_in, half_down = wi.at[:, q], wd.at[q]
    remote(half_in, half_in, out_sem, wr_sem.at[0], tp=sib).wait_send()
    remote(half_down, half_down, out_sem, wr_sem.at[0], tp=sib).wait_send()
    most = x.at[pl.ds(0, gs - 1)]
    remote(most, most, out_sem, dr_sem.at[0], tp=sib).wait_send()
    remote(most, most, out_sem, br_sem.at[0], tp=sib).wait_send()


def shards(tokens, norm_gain, group_prob, route_logits, expert_ids, w_gate, w_up, w_down):
    width = lax.axis_size("ep")
    n_tp = lax.axis_size("tp")
    count, dmodel = tokens.shape
    topk = expert_ids.shape[1]
    ff = w_gate.shape[2]
    cap = count // GROUPS
    gs = width // GROUPS
    hbm = pl.BlockSpec(memory_space=pltpu.HBM)
    bf, f32 = jnp.bfloat16, jnp.float32
    dma = pltpu.SemaphoreType.DMA
    return pl.pallas_call(
        functools.partial(kernel, width, n_tp),
        out_shape=pltpu.VMEM((count, dmodel), bf),
        in_specs=[hbm] * 8,
        out_specs=pl.BlockSpec(memory_space=pltpu.VMEM),
        scratch_shapes=[
            pltpu.VMEM((count, dmodel), bf),
            pltpu.VMEM((1, dmodel), f32),
            pltpu.VMEM((1, count), f32),
            pltpu.VMEM((topk, count), f32),
            pltpu.VMEM((topk, count), jnp.int32),
            pltpu.VMEM((2, n_tp, dmodel, ff), bf),
            pltpu.VMEM((n_tp, ff, dmodel), bf),
            pltpu.VMEM((cap, dmodel), bf),
            pltpu.VMEM((cap, 128), f32),
            pltpu.VMEM((cap, 128), f32),
            pltpu.VMEM((gs, cap, dmodel), bf),
            pltpu.VMEM((gs, cap, dmodel), bf),
            pltpu.VMEM((gs, cap, dmodel), bf),
            pltpu.VMEM((cap, dmodel), bf),
            pltpu.VMEM((2, cap, dmodel), bf),
            pltpu.VMEM((n_tp, cap, dmodel), bf),
            dma, dma((2,)), dma, dma((2 * CHUNKS,)), dma((CHUNKS,)), dma,
            dma((CHUNKS + 1,)), dma((CHUNKS,)), dma((CHUNKS + 1,)), dma((CHUNKS,)),
        ],
        compiler_params=pltpu.CompilerParams(collective_id=0, has_side_effects=True),
        name="expert_mixture",
    )(
        tokens, norm_gain.reshape(1, dmodel), group_prob.reshape(1, count), route_logits.T,
        expert_ids.T, w_gate, w_up, w_down,
    )


def solution(mesh):
    in_specs = (
        P(("grp", "ep"), None),
        P(),
        P(("grp", "ep")),
        P(("grp", "ep"), None),
        P(("grp", "ep"), None),
        P("ep", None, "tp"),
        P("ep", None, "tp"),
        P("ep", "tp", None),
    )
    out_specs = P(("grp", "ep"), None)
    return jax.shard_map(shards, mesh=mesh, in_specs=in_specs, out_specs=out_specs, check_vma=False)
```

```python
import functools

import jax
import jax.numpy as jnp
from jax import lax
from jax.experimental import pallas as pl
from jax.experimental.pallas import tpu as pltpu
from jax.sharding import PartitionSpec as P

GROUPS = 2
CHUNKS = 4
FIRST = 2
HOLD = 3
TWICE = 1
MESH = pl.DeviceIdType.MESH


def kernel(
    width, n_tp,
    tok_hbm, gain_hbm, prob_hbm, logit_hbm, ids_hbm, wg_hbm, wu_hbm, wd_hbm,
    out_ref,
    tok, gain, prob, logit, ids, wi, wd, send, wsend, wroot, x, outs, back, red, got, mixed,
    in_sem, wl_sem, out_sem, wr_sem, xr_sem, vr_sem, dr_sem, br_sem, cr_sem, mr_sem, ready_sem, go_sem,
):
    e = lax.axis_index("ep")
    q = lax.axis_index("tp")
    sib = n_tp - 1 - q
    gs = width // GROUPS
    count, dmodel = tok.shape
    cap = count // GROUPS
    topk = ids.shape[0]
    block = e // gs
    local = e % gs
    base = block * gs
    partner = (e + gs) % width
    far = gs - 1 - local
    cross = q == n_tp - 1
    own = q != n_tp - 1
    group = (block + q) % GROUPS
    cw = dmodel // CHUNKS
    ff = wi.shape[3]
    f32, bf = jnp.float32, jnp.bfloat16
    split = cross & (block != 0)
    late = own & (block != 0)
    held = split & (local < 1)
    end = CHUNKS - TWICE

    def cols(c):
        return pl.ds(c * cw, cw)

    def peer(j):
        return base + (local + j) % gs

    def remote(src, dst, ss, rs, **where):
        return pltpu.make_async_remote_copy(
            src_ref=src, dst_ref=dst, send_sem=ss, recv_sem=rs,
            device_id=where, device_id_type=MESH,
        )

    smalls = [
        pltpu.make_async_copy(src, dst, in_sem)
        for src, dst in [
            (tok_hbm, tok), (gain_hbm, gain), (prob_hbm, prob), (logit_hbm, logit), (ids_hbm, ids)
        ]
    ]
    for c in smalls:
        c.start()
    loads = [
        pltpu.make_async_copy(src.at[0], dst, wl_sem.at[i // 2])
        for i, (src, dst) in enumerate([(wg_hbm, wi.at[0, q]), (wu_hbm, wi.at[1, q]), (wd_hbm, wd.at[q])])
    ]
    for c in loads:
        c.start()

    barrier = pltpu.get_barrier_semaphore()

    @pl.when(cross)
    def _():
        pl.semaphore_signal(barrier, inc=1, device_id={"ep": partner}, device_id_type=MESH)

    @pl.when(jnp.logical_not(late))
    def _():
        for j in range(1, gs):
            pl.semaphore_signal(barrier, inc=1, device_id={"ep": peer(j)}, device_id_type=MESH)

    pl.semaphore_signal(barrier, inc=1, device_id={"tp": sib}, device_id_type=MESH)

    for c in smalls:
        c.wait()
    values = tok[...].astype(f32)
    scale = lax.rsqrt(jnp.mean(values * values, axis=-1, keepdims=True) + 1e-06)
    normed = (values * scale * gain[...]).astype(bf)
    idv = ids[...]
    first = idv[0:1, :]
    grow = jnp.zeros((1, count), f32)
    for g in range(1, GROUPS):
        grow = grow + jnp.where(first >= g * gs, 1.0, 0.0)
    t_row = lax.broadcasted_iota(jnp.int32, (count, count), 0)
    t_col = lax.broadcasted_iota(jnp.int32, (count, count), 1)
    gfull = jnp.broadcast_to(grow, (count, count))
    gcol = jnp.sum(jnp.where(t_row == t_col, gfull, 0.0), axis=1, keepdims=True)
    same = jnp.where(gfull == gcol, 1.0, 0.0)
    pos_row = jnp.sum(jnp.where(t_row < t_col, same, 0.0), axis=0, keepdims=True)
    pos_col = jnp.sum(jnp.where(t_col < t_row, same, 0.0), axis=1, keepdims=True)
    r_io = lax.broadcasted_iota(jnp.int32, (cap, count), 0).astype(f32)
    place = jnp.where((pos_row == r_io) & (grow == group.astype(f32)), 1.0, 0.0)
    rows = jnp.dot(place.astype(bf), normed, preferred_element_type=f32).astype(bf)

    @pl.when(cross)
    def _():
        send[...] = rows

    @pl.when(own)
    def _():
        x[local] = rows

    pl.semaphore_wait(barrier, jnp.where(late, 1, jnp.where(cross, gs + 1, gs)))

    def across(c):
        return remote(send.at[:, cols(c)], x.at[local, :, cols(c)], out_sem, xr_sem.at[c], ep=partner)

    def spread(j, c):
        part = x.at[local, :, cols(c)]
        return remote(part, part, out_sem, dr_sem.at[jnp.where(split & (local >= FIRST), CHUNKS, c)], ep=peer(j))

    @pl.when(cross)
    def _():
        for c in range(CHUNKS):
            across(c).start()

    @pl.when(split)
    def _():
        for j in range(1, gs):
            pl.semaphore_signal(ready_sem, inc=1, device_id={"ep": peer(j)}, device_id_type=MESH)

    def spread_all():
        for c in range(CHUNKS):
            for j in [*range(1, gs, 2), *range(2, gs, 2)]:
                spread(j, c).start()

    @pl.when(own & (block == 0))
    def _():
        spread_all()

    def swap_in(h, c):
        part = wi.at[:, h, cols(c)]
        return remote(part, part, out_sem, wr_sem.at[c], tp=sib)

    def swap_down(h, c):
        part = wd.at[h, :, cols(c)]
        return remote(part, part, out_sem, wr_sem.at[CHUNKS + c], tp=sib)

    for c in loads[:2]:
        c.wait()
    for c in range(CHUNKS):
        swap_in(q, c).start()
    loads[2].wait()
    for c in range(CHUNKS):
        swap_down(q, c).start()

    expw = jnp.exp(logit[...])
    route = prob[...] * expw / jnp.sum(expw, axis=0, keepdims=True)
    k_io = lax.broadcasted_iota(jnp.int32, (128, count), 0)
    column = jnp.where(k_io < gs - 1, k_io + jnp.where(k_io >= far, 1, 0), far)
    column = jnp.where(k_io < gs, column, -1)
    within = idv - jnp.where(grow > 0.0, gs, 0)
    wtok = jnp.zeros((128, count), f32)
    for k in range(topk):
        wtok = wtok + jnp.where(within[k : k + 1, :] == column, route[k : k + 1, :], 0.0)

    def slots_of(placed):
        return lax.dot_general(
            placed, wtok, (((1,), (1,)), ((), ())),
            precision=lax.Precision.HIGHEST, preferred_element_type=f32,
        )

    def weights_across():
        return remote(wsend, wroot, out_sem, vr_sem, ep=partner)

    there = jnp.where((pos_row == r_io) & (grow == (1 - block).astype(f32)), 1.0, 0.0)
    wsend[...] = slots_of(there)

    @pl.when(cross)
    def _():
        weights_across().start()

    @pl.when(own)
    def _():
        wroot[...] = slots_of(place)

    s_io = lax.broadcasted_iota(jnp.int32, (count, count), 1).astype(f32)
    role = jnp.where(gcol == block.astype(f32), 0.0, 1.0)
    unplace = jnp.where(s_io == role * cap + pos_col, 1.0, 0.0).astype(bf)

    @pl.when(late)
    def _():
        pl.semaphore_wait(go_sem, 1)
        for c in range(HOLD):
            swap_in(sib, c).wait_recv()
        spread_all()

    @pl.when(cross)
    def _():
        for c in range(CHUNKS):
            across(c).wait_recv()
            for j in [*range(1, gs, 2), *range(2, gs, 2)]:
                spread(j, c).start()
            if c == 0:

                @pl.when(split)
                def _():
                    pl.semaphore_wait(ready_sem, gs - 1)
                    pl.semaphore_signal(go_sem, inc=1, device_id={"tp": sib}, device_id_type=MESH)

    def landed(b, lo, hi, c):
        inside = (local >= lo) & (local < hi)

        def take(n):
            part = x.at[pl.ds(lo, n), :, cols(c)] if b == 0 else x.at[pl.ds(lo, n)]
            sem = dr_sem.at[c if b == 0 else CHUNKS]
            remote(part, part, out_sem, sem, tp=sib).wait_recv()

        if b > 0 and c > 0:
            return
        if hi - lo == gs:
            take(gs - 1)
            return
        if hi - lo > 1:

            @pl.when(inside)
            def _():
                take(hi - lo - 1)

        @pl.when(jnp.logical_not(inside))
        def _():
            take(hi - lo)

    def give(r, c):
        return remote(
            outs.at[r, :, cols(c)], back.at[local, :, cols(c)], out_sem, br_sem.at[c], ep=base + r
        )

    def both(src, place, c, sem, to):
        dst = got.at[place, :, cols(c)]
        early = place == 1 and c == end
        remote(src, dst, sem, cr_sem.at[CHUNKS if early else c], ep=to).start()
        if c >= end and place == 0:
            remote(src, dst, out_sem, cr_sem.at[c], ep=to, tp=sib).start()

    def send_direct(r, c):
        both(outs.at[r, :, cols(c)], 1, c, out_sem, (base + r + gs) % width)

    def experts(b, lo, hi):
        n = (hi - lo) * cap
        gates = [jnp.zeros((n, ff), f32)] * n_tp
        ups = [jnp.zeros((n, ff), f32)] * n_tp
        for c in range(CHUNKS):
            landed(b, lo, hi, c)
            if b == 0 and c >= HOLD:
                swap_in(sib, c).wait_recv()
            elif b == 0:

                @pl.when(jnp.logical_not(late))
                def _():
                    swap_in(sib, c).wait_recv()

            k = slice(c * cw, (c + 1) * cw)
            xc = x[lo:hi, :, k].reshape(n, cw)
            for h in range(n_tp):
                gates[h] = gates[h] + jnp.dot(xc, wi[0, h, k], preferred_element_type=f32)
                ups[h] = ups[h] + jnp.dot(xc, wi[1, h, k], preferred_element_type=f32)
        acts = [((g / (1.0 + jnp.exp(-g))) * u).astype(bf) for g, u in zip(gates, ups)]

        def down(c):
            if b == 0:
                swap_down(sib, c).wait_recv()
            k = slice(c * cw, (c + 1) * cw)
            total = jnp.dot(acts[0], wd[0, :, k], preferred_element_type=f32)
            for h in range(1, n_tp):
                total = total + jnp.dot(acts[h], wd[h, :, k], preferred_element_type=f32)
            return total.astype(bf).reshape(hi - lo, cap, cw)

        ready = down(0)
        for c in range(CHUNKS):
            k = slice(c * cw, (c + 1) * cw)
            outs[lo:hi, :, k] = ready
            if c + 1 < CHUNKS:
                ready = down(c + 1)
            for r in range(lo, hi):

                @pl.when(local == r)
                def _():
                    back[r, :, k] = outs[r, :, k]

                @pl.when((local != r) & (own | (far != r)))
                def _():
                    give(r, c).start()

                @pl.when(cross & (far == r) & jnp.logical_not(held))
                def _():
                    send_direct(r, c)

    @pl.when(split)
    def _():
        experts(0, 0, FIRST)
        experts(1, FIRST, gs)

    @pl.when(jnp.logical_not(split))
    def _():
        experts(0, 0, gs)

    def share(c):
        part = mixed.at[q, :, cols(c)]
        return remote(part, part, out_sem, mr_sem.at[c], tp=sib)

    def shared(c):
        part = mixed.at[sib, :, cols(c)]
        return remote(part, part, out_sem, mr_sem.at[c], tp=sib)

    @pl.when(cross)
    def _():
        weights_across().wait_recv()

    wv = wroot[...]
    near = [i + jnp.where(i >= far, 1, 0) for i in range(gs - 1)]
    for c in range(CHUNKS):
        k = slice(c * cw, (c + 1) * cw)

        def returned(n):
            part = back.at[pl.ds(0, n), :, cols(c)]
            remote(part, part, out_sem, br_sem.at[c], tp=sib).wait_recv()

        @pl.when(cross)
        def _():
            returned(gs - 2)

        @pl.when(own)
        def _():
            returned(gs - 1)

        acc = wv[:, 0:1] * back[near[0], :, k].astype(f32)
        for i in range(1, gs - 1):
            acc = acc + wv[:, i : i + 1] * back[near[i], :, k].astype(f32)

        @pl.when(cross)
        def _():
            red[:, k] = acc.astype(bf)
            both(red.at[:, cols(c)], 0, c, out_sem, partner)

        @pl.when(own)
        def _():
            last = wv[:, gs - 1 : gs] * back[far, :, k].astype(f32)
            mixed[0, :, k] = (acc + last).astype(bf)
            share(c).start()

    @pl.when(held)
    def _():
        for c in range(CHUNKS):
            send_direct(far, c)

    spot = got.at[1, :, cols(end)]

    def pass_on():
        return remote(spot, spot, out_sem, cr_sem.at[CHUNKS], tp=sib)

    def arrived(c):
        k = slice(c * cw, (c + 1) * cw)
        part = got.at[0, :, cols(c)] if c == end else got.at[:, :, cols(c)]
        remote(part, part, out_sem, cr_sem.at[c], tp=sib).wait_recv()
        last = wsend[:, gs - 1 : gs] * got[1, :, k].astype(f32)
        mixed[n_tp - 1, :, k] = (got[0, :, k].astype(f32) + last).astype(bf)

    def restore(c):
        k = slice(c * cw, (c + 1) * cw)
        slots = mixed[:, :, k].reshape(count, cw)
        out_ref[:, k] = jnp.dot(unplace, slots, preferred_element_type=f32).astype(bf)

    @pl.when(cross)
    def _():
        pass_on().wait_recv()
        pass_on().start()
        for c in range(CHUNKS):
            arrived(c)
            if c < end:
                share(c).start()
            if c == end - 1:
                for d in range(c):
                    shared(d).wait_recv()
                    restore(d)
            if c >= end:
                shared(c - 1).wait_recv()
                restore(c - 1)
        shared(CHUNKS - 1).wait_recv()
        restore(CHUNKS - 1)

    @pl.when(own)
    def _():
        for c in range(end):
            shared(c).wait_recv()
            restore(c)
        pass_on().wait_recv()
        arrived(end)
        restore(end)

    @pl.when(cross)
    def _():
        weights_across().wait_send()
        remote(send, send, out_sem, xr_sem.at[0], tp=sib).wait_send()
        remote(red, red, out_sem, cr_sem.at[0], tp=sib).wait_send()
        twice = got.at[:, :, pl.ds(end * cw, TWICE * cw)]
        remote(twice, twice, out_sem, cr_sem.at[0], tp=sib).wait_send()
        most_mixed = mixed.at[q, :, pl.ds(0, end * cw)]
        remote(most_mixed, most_mixed, out_sem, mr_sem.at[0], tp=sib).wait_send()

    @pl.when(own)
    def _():
        remote(mixed.at[q], mixed.at[q], out_sem, mr_sem.at[0], tp=sib).wait_send()

    half_in, half_down = wi.at[:, q], wd.at[q]
    remote(half_in, half_in, out_sem, wr_sem.at[0], tp=sib).wait_send()
    remote(half_down, half_down, out_sem, wr_sem.at[0], tp=sib).wait_send()
    most = x.at[pl.ds(0, gs - 1)]
    remote(most, most, out_sem, dr_sem.at[0], tp=sib).wait_send()
    remote(most, most, out_sem, br_sem.at[0], tp=sib).wait_send()


def shards(tokens, norm_gain, group_prob, route_logits, expert_ids, w_gate, w_up, w_down):
    width = lax.axis_size("ep")
    n_tp = lax.axis_size("tp")
    count, dmodel = tokens.shape
    topk = expert_ids.shape[1]
    ff = w_gate.shape[2]
    cap = count // GROUPS
    gs = width // GROUPS
    hbm = pl.BlockSpec(memory_space=pltpu.HBM)
    bf, f32 = jnp.bfloat16, jnp.float32
    dma = pltpu.SemaphoreType.DMA
    return pl.pallas_call(
        functools.partial(kernel, width, n_tp),
        out_shape=pltpu.VMEM((count, dmodel), bf),
        in_specs=[hbm] * 8,
        out_specs=pl.BlockSpec(memory_space=pltpu.VMEM),
        scratch_shapes=[
            pltpu.VMEM((count, dmodel), bf),
            pltpu.VMEM((1, dmodel), f32),
            pltpu.VMEM((1, count), f32),
            pltpu.VMEM((topk, count), f32),
            pltpu.VMEM((topk, count), jnp.int32),
            pltpu.VMEM((2, n_tp, dmodel, ff), bf),
            pltpu.VMEM((n_tp, ff, dmodel), bf),
            pltpu.VMEM((cap, dmodel), bf),
            pltpu.VMEM((cap, 128), f32),
            pltpu.VMEM((cap, 128), f32),
            pltpu.VMEM((gs, cap, dmodel), bf),
            pltpu.VMEM((gs, cap, dmodel), bf),
            pltpu.VMEM((gs, cap, dmodel), bf),
            pltpu.VMEM((cap, dmodel), bf),
            pltpu.VMEM((2, cap, dmodel), bf),
            pltpu.VMEM((n_tp, cap, dmodel), bf),
            dma, dma((2,)), dma, dma((2 * CHUNKS,)), dma((CHUNKS,)), dma,
            dma((CHUNKS + 1,)), dma((CHUNKS,)), dma((CHUNKS + 1,)), dma((CHUNKS,)),
            pltpu.SemaphoreType.REGULAR, pltpu.SemaphoreType.REGULAR,
        ],
        compiler_params=pltpu.CompilerParams(collective_id=0, has_side_effects=True),
        name="expert_mixture",
    )(
        tokens, norm_gain.reshape(1, dmodel), group_prob.reshape(1, count), route_logits.T,
        expert_ids.T, w_gate, w_up, w_down,
    )


def solution(mesh):
    in_specs = (
        P(("grp", "ep"), None),
        P(),
        P(("grp", "ep")),
        P(("grp", "ep"), None),
        P(("grp", "ep"), None),
        P("ep", None, "tp"),
        P("ep", None, "tp"),
        P("ep", "tp", None),
    )
    out_specs = P(("grp", "ep"), None)
    return jax.shard_map(shards, mesh=mesh, in_specs=in_specs, out_specs=out_specs, check_vma=False)
```

```python
import functools

import jax
import jax.numpy as jnp
from jax import lax
from jax.experimental import pallas as pl
from jax.experimental.pallas import tpu as pltpu
from jax.sharding import PartitionSpec as P

GROUPS = 2
CHUNKS = 4
FIRST = 2
HOLD = 3
TWICE = 1
MESH = pl.DeviceIdType.MESH


def kernel(
    width, n_tp,
    tok_hbm, gain_hbm, prob_hbm, logit_hbm, ids_hbm, wg_hbm, wu_hbm, wd_hbm,
    out_ref,
    tok, gain, prob, logit, ids, wi, wd, send, wsend, wroot, x, outs, back, red, got, mixed,
    in_sem, wl_sem, out_sem, wr_sem, xr_sem, vr_sem, dr_sem, br_sem, cr_sem, mr_sem, ready_sem, go_sem,
):
    e = lax.axis_index("ep")
    q = lax.axis_index("tp")
    sib = n_tp - 1 - q
    gs = width // GROUPS
    count, dmodel = tok.shape
    cap = count // GROUPS
    topk = ids.shape[0]
    block = e // gs
    local = e % gs
    base = block * gs
    partner = (e + gs) % width
    far = gs - 1 - local
    cross = q == n_tp - 1
    own = q != n_tp - 1
    group = (block + q) % GROUPS
    cw = dmodel // CHUNKS
    ff = wi.shape[3]
    f32, bf = jnp.float32, jnp.bfloat16
    split = cross & (block != 0)
    late = own & (block != 0)
    held = split & (local < 1)
    end = CHUNKS - TWICE

    def cols(c):
        return pl.ds(c * cw, cw)

    def peer(j):
        return base + (local + j) % gs

    def remote(src, dst, ss, rs, **where):
        return pltpu.make_async_remote_copy(
            src_ref=src, dst_ref=dst, send_sem=ss, recv_sem=rs,
            device_id=where, device_id_type=MESH,
        )

    smalls = [
        pltpu.make_async_copy(src, dst, in_sem)
        for src, dst in [
            (tok_hbm, tok), (gain_hbm, gain), (prob_hbm, prob), (logit_hbm, logit), (ids_hbm, ids)
        ]
    ]
    for c in smalls:
        c.start()
    loads = [
        pltpu.make_async_copy(src.at[0], dst, wl_sem.at[i // 2])
        for i, (src, dst) in enumerate([(wg_hbm, wi.at[0, q]), (wu_hbm, wi.at[1, q]), (wd_hbm, wd.at[q])])
    ]
    for c in loads:
        c.start()

    barrier = pltpu.get_barrier_semaphore()

    @pl.when(cross)
    def _():
        pl.semaphore_signal(barrier, inc=1, device_id={"ep": partner}, device_id_type=MESH)

    @pl.when(jnp.logical_not(late))
    def _():
        for j in range(1, gs):
            pl.semaphore_signal(barrier, inc=1, device_id={"ep": peer(j)}, device_id_type=MESH)

    pl.semaphore_signal(barrier, inc=1, device_id={"tp": sib}, device_id_type=MESH)

    for c in smalls:
        c.wait()
    values = tok[...].astype(f32)
    scale = lax.rsqrt(jnp.mean(values * values, axis=-1, keepdims=True) + 1e-06)
    normed = (values * scale * gain[...]).astype(bf)
    idv = ids[...]
    first = idv[0:1, :]
    grow = jnp.zeros((1, count), f32)
    for g in range(1, GROUPS):
        grow = grow + jnp.where(first >= g * gs, 1.0, 0.0)
    t_row = lax.broadcasted_iota(jnp.int32, (count, count), 0)
    t_col = lax.broadcasted_iota(jnp.int32, (count, count), 1)
    gfull = jnp.broadcast_to(grow, (count, count))
    gcol = jnp.sum(jnp.where(t_row == t_col, gfull, 0.0), axis=1, keepdims=True)
    same = jnp.where(gfull == gcol, 1.0, 0.0)
    pos_row = jnp.sum(jnp.where(t_row < t_col, same, 0.0), axis=0, keepdims=True)
    pos_col = jnp.sum(jnp.where(t_col < t_row, same, 0.0), axis=1, keepdims=True)
    r_io = lax.broadcasted_iota(jnp.int32, (cap, count), 0).astype(f32)
    place = jnp.where((pos_row == r_io) & (grow == group.astype(f32)), 1.0, 0.0)
    rows = jnp.dot(place.astype(bf), normed, preferred_element_type=f32).astype(bf)

    @pl.when(cross)
    def _():
        send[...] = rows

    @pl.when(own)
    def _():
        x[local] = rows

    pl.semaphore_wait(barrier, jnp.where(late, 1, jnp.where(cross, gs + 1, gs)))

    def across(c):
        return remote(send.at[:, cols(c)], x.at[local, :, cols(c)], out_sem, xr_sem.at[c], ep=partner)

    def spread(j, c):
        part = x.at[local, :, cols(c)]
        return remote(part, part, out_sem, dr_sem.at[jnp.where(split & (local >= FIRST), CHUNKS, c)], ep=peer(j))

    @pl.when(cross)
    def _():
        for c in range(CHUNKS):
            across(c).start()

    @pl.when(split)
    def _():
        for j in range(1, gs):
            pl.semaphore_signal(ready_sem, inc=1, device_id={"ep": peer(j)}, device_id_type=MESH)

    def spread_all():
        for c in range(CHUNKS):
            for j in [*range(1, gs, 2), *range(2, gs, 2)]:
                spread(j, c).start()

    @pl.when(own & (block == 0))
    def _():
        spread_all()

    def swap_in(h, c):
        part = wi.at[:, h, cols(c)]
        return remote(part, part, out_sem, wr_sem.at[c], tp=sib)

    def swap_down(h, c):
        part = wd.at[h, :, cols(c)]
        return remote(part, part, out_sem, wr_sem.at[CHUNKS + c], tp=sib)

    for c in loads[:2]:
        c.wait()
    for c in range(CHUNKS):
        swap_in(q, c).start()
    loads[2].wait()
    for c in range(CHUNKS):
        swap_down(q, c).start()

    expw = jnp.exp(logit[...])
    route = prob[...] * expw / jnp.sum(expw, axis=0, keepdims=True)
    k_io = lax.broadcasted_iota(jnp.int32, (128, count), 0)
    column = jnp.where(k_io < gs - 1, k_io + jnp.where(k_io >= far, 1, 0), far)
    column = jnp.where(k_io < gs, column, -1)
    within = idv - jnp.where(grow > 0.0, gs, 0)
    wtok = jnp.zeros((128, count), f32)
    for k in range(topk):
        wtok = wtok + jnp.where(within[k : k + 1, :] == column, route[k : k + 1, :], 0.0)

    def slots_of(placed):
        return lax.dot_general(
            placed, wtok, (((1,), (1,)), ((), ())),
            precision=lax.Precision.HIGHEST, preferred_element_type=f32,
        )

    def weights_across():
        return remote(wsend, wroot, out_sem, vr_sem, ep=partner)

    there = jnp.where((pos_row == r_io) & (grow == (1 - block).astype(f32)), 1.0, 0.0)
    wsend[...] = slots_of(there)

    @pl.when(cross)
    def _():
        weights_across().start()

    @pl.when(own)
    def _():
        wroot[...] = slots_of(place)

    s_io = lax.broadcasted_iota(jnp.int32, (count, count), 1).astype(f32)
    role = jnp.where(gcol == block.astype(f32), 0.0, 1.0)
    unplace = jnp.where(s_io == role * cap + pos_col, 1.0, 0.0).astype(bf)

    @pl.when(late)
    def _():
        pl.semaphore_wait(go_sem, 1)
        for c in range(HOLD):
            swap_in(sib, c).wait_recv()
        spread_all()

    @pl.when(cross)
    def _():
        for c in range(CHUNKS):
            across(c).wait_recv()
            for j in [*range(1, gs, 2), *range(2, gs, 2)]:
                spread(j, c).start()
            if c == 0:

                @pl.when(split)
                def _():
                    pl.semaphore_wait(ready_sem, gs - 1)
                    pl.semaphore_signal(go_sem, inc=1, device_id={"tp": sib}, device_id_type=MESH)

    def landed(b, lo, hi, c):
        inside = (local >= lo) & (local < hi)

        def take(n):
            part = x.at[pl.ds(lo, n), :, cols(c)] if b == 0 else x.at[pl.ds(lo, n)]
            sem = dr_sem.at[c if b == 0 else CHUNKS]
            remote(part, part, out_sem, sem, tp=sib).wait_recv()

        if b > 0 and c > 0:
            return
        if hi - lo == gs:
            take(gs - 1)
            return
        if hi - lo > 1:

            @pl.when(inside)
            def _():
                take(hi - lo - 1)

        @pl.when(jnp.logical_not(inside))
        def _():
            take(hi - lo)

    def give(r, c):
        return remote(
            outs.at[r, :, cols(c)], back.at[local, :, cols(c)], out_sem, br_sem.at[c], ep=base + r
        )

    def both(src, place, c, sem, to):
        dst = got.at[place, :, cols(c)]
        early = place == 1 and c == end
        remote(src, dst, sem, cr_sem.at[CHUNKS if early else c], ep=to).start()
        if c >= end and place == 0:
            remote(src, dst, out_sem, cr_sem.at[c], ep=to, tp=sib).start()

    def send_direct(r, c):
        both(outs.at[r, :, cols(c)], 1, c, out_sem, (base + r + gs) % width)

    def experts(b, lo, hi):
        n = (hi - lo) * cap
        gates = [jnp.zeros((n, ff), f32)] * n_tp
        ups = [jnp.zeros((n, ff), f32)] * n_tp
        for c in range(CHUNKS):
            landed(b, lo, hi, c)
            if b == 0 and c >= HOLD:
                swap_in(sib, c).wait_recv()
            elif b == 0:

                @pl.when(jnp.logical_not(late))
                def _():
                    swap_in(sib, c).wait_recv()

            k = slice(c * cw, (c + 1) * cw)
            xc = x[lo:hi, :, k].reshape(n, cw)
            for h in range(n_tp):
                gates[h] = gates[h] + jnp.dot(xc, wi[0, h, k], preferred_element_type=f32)
                ups[h] = ups[h] + jnp.dot(xc, wi[1, h, k], preferred_element_type=f32)
        acts = [((g / (1.0 + jnp.exp(-g))) * u).astype(bf) for g, u in zip(gates, ups)]

        def down(c):
            if b == 0:
                swap_down(sib, c).wait_recv()
            k = slice(c * cw, (c + 1) * cw)
            total = jnp.dot(acts[0], wd[0, :, k], preferred_element_type=f32)
            for h in range(1, n_tp):
                total = total + jnp.dot(acts[h], wd[h, :, k], preferred_element_type=f32)
            return total.astype(bf).reshape(hi - lo, cap, cw)

        ready = down(0)
        for c in range(CHUNKS):
            k = slice(c * cw, (c + 1) * cw)
            outs[lo:hi, :, k] = ready
            if c + 1 < CHUNKS:
                ready = down(c + 1)
            for r in range(lo, hi):

                @pl.when(local == r)
                def _():
                    back[r, :, k] = outs[r, :, k]

                @pl.when((local != r) & (own | (far != r)))
                def _():
                    give(r, c).start()

                @pl.when(cross & (far == r) & jnp.logical_not(held))
                def _():
                    send_direct(r, c)

    @pl.when(split)
    def _():
        experts(0, 0, FIRST)
        experts(1, FIRST, gs)

    @pl.when(jnp.logical_not(split))
    def _():
        experts(0, 0, gs)

    def share(c):
        part = mixed.at[q, :, cols(c)]
        return remote(part, part, out_sem, mr_sem.at[c], tp=sib)

    def shared(c):
        part = mixed.at[sib, :, cols(c)]
        return remote(part, part, out_sem, mr_sem.at[c], tp=sib)

    @pl.when(cross)
    def _():
        weights_across().wait_recv()

    wv = wroot[...]
    near = [i + jnp.where(i >= far, 1, 0) for i in range(gs - 1)]
    for c in range(CHUNKS):
        k = slice(c * cw, (c + 1) * cw)

        def returned(n):
            part = back.at[pl.ds(0, n), :, cols(c)]
            remote(part, part, out_sem, br_sem.at[c], tp=sib).wait_recv()

        @pl.when(cross)
        def _():
            returned(gs - 2)

        @pl.when(own)
        def _():
            returned(gs - 1)

        acc = wv[:, 0:1] * back[near[0], :, k].astype(f32)
        for i in range(1, gs - 1):
            acc = acc + wv[:, i : i + 1] * back[near[i], :, k].astype(f32)

        @pl.when(cross)
        def _():
            red[:, k] = acc.astype(bf)
            both(red.at[:, cols(c)], 0, c, out_sem, partner)

        @pl.when(own)
        def _():
            last = wv[:, gs - 1 : gs] * back[far, :, k].astype(f32)
            mixed[0, :, k] = (acc + last).astype(bf)
            share(c).start()

    @pl.when(held)
    def _():
        for c in range(CHUNKS):
            send_direct(far, c)

    spot = got.at[1, :, cols(end)]

    def pass_on():
        return remote(spot, spot, out_sem, cr_sem.at[CHUNKS], tp=sib)

    def arrived(c):
        k = slice(c * cw, (c + 1) * cw)
        part = got.at[0, :, cols(c)] if c == end else got.at[:, :, cols(c)]
        remote(part, part, out_sem, cr_sem.at[c], tp=sib).wait_recv()
        last = wsend[:, gs - 1 : gs] * got[1, :, k].astype(f32)
        mixed[n_tp - 1, :, k] = (got[0, :, k].astype(f32) + last).astype(bf)

    def restore(c, n=1):
        k = slice(c * cw, (c + n) * cw)
        slots = mixed[:, :, k].reshape(count, n * cw)
        out_ref[:, k] = jnp.dot(unplace, slots, preferred_element_type=f32).astype(bf)

    @pl.when(cross)
    def _():
        pass_on().wait_recv()
        pass_on().start()
        for c in range(CHUNKS):
            arrived(c)
            if c < end:
                share(c).start()
            if c == end - 1:
                for d in range(c):
                    shared(d).wait_recv()
                    restore(d)
        shared(end - 1).wait_recv()
        shared(end).wait_recv()
        restore(end - 1, 2)

    @pl.when(own)
    def _():
        for c in range(end - 1):
            shared(c).wait_recv()
            restore(c)
        shared(end - 1).wait_recv()
        pass_on().wait_recv()
        arrived(end)
        restore(end - 1, 2)

    @pl.when(cross)
    def _():
        weights_across().wait_send()
        remote(send, send, out_sem, xr_sem.at[0], tp=sib).wait_send()
        remote(red, red, out_sem, cr_sem.at[0], tp=sib).wait_send()
        twice = got.at[:, :, pl.ds(end * cw, TWICE * cw)]
        remote(twice, twice, out_sem, cr_sem.at[0], tp=sib).wait_send()
        most_mixed = mixed.at[q, :, pl.ds(0, end * cw)]
        remote(most_mixed, most_mixed, out_sem, mr_sem.at[0], tp=sib).wait_send()

    @pl.when(own)
    def _():
        remote(mixed.at[q], mixed.at[q], out_sem, mr_sem.at[0], tp=sib).wait_send()

    half_in, half_down = wi.at[:, q], wd.at[q]
    remote(half_in, half_in, out_sem, wr_sem.at[0], tp=sib).wait_send()
    remote(half_down, half_down, out_sem, wr_sem.at[0], tp=sib).wait_send()
    most = x.at[pl.ds(0, gs - 1)]
    remote(most, most, out_sem, dr_sem.at[0], tp=sib).wait_send()
    remote(most, most, out_sem, br_sem.at[0], tp=sib).wait_send()


def shards(tokens, norm_gain, group_prob, route_logits, expert_ids, w_gate, w_up, w_down):
    width = lax.axis_size("ep")
    n_tp = lax.axis_size("tp")
    count, dmodel = tokens.shape
    topk = expert_ids.shape[1]
    ff = w_gate.shape[2]
    cap = count // GROUPS
    gs = width // GROUPS
    hbm = pl.BlockSpec(memory_space=pltpu.HBM)
    bf, f32 = jnp.bfloat16, jnp.float32
    dma = pltpu.SemaphoreType.DMA
    return pl.pallas_call(
        functools.partial(kernel, width, n_tp),
        out_shape=pltpu.VMEM((count, dmodel), bf),
        in_specs=[hbm] * 8,
        out_specs=pl.BlockSpec(memory_space=pltpu.VMEM),
        scratch_shapes=[
            pltpu.VMEM((count, dmodel), bf),
            pltpu.VMEM((1, dmodel), f32),
            pltpu.VMEM((1, count), f32),
            pltpu.VMEM((topk, count), f32),
            pltpu.VMEM((topk, count), jnp.int32),
            pltpu.VMEM((2, n_tp, dmodel, ff), bf),
            pltpu.VMEM((n_tp, ff, dmodel), bf),
            pltpu.VMEM((cap, dmodel), bf),
            pltpu.VMEM((cap, 128), f32),
            pltpu.VMEM((cap, 128), f32),
            pltpu.VMEM((gs, cap, dmodel), bf),
            pltpu.VMEM((gs, cap, dmodel), bf),
            pltpu.VMEM((gs, cap, dmodel), bf),
            pltpu.VMEM((cap, dmodel), bf),
            pltpu.VMEM((2, cap, dmodel), bf),
            pltpu.VMEM((n_tp, cap, dmodel), bf),
            dma, dma((2,)), dma, dma((2 * CHUNKS,)), dma((CHUNKS,)), dma,
            dma((CHUNKS + 1,)), dma((CHUNKS,)), dma((CHUNKS + 1,)), dma((CHUNKS,)),
            pltpu.SemaphoreType.REGULAR, pltpu.SemaphoreType.REGULAR,
        ],
        compiler_params=pltpu.CompilerParams(collective_id=0, has_side_effects=True),
        name="expert_mixture",
    )(
        tokens, norm_gain.reshape(1, dmodel), group_prob.reshape(1, count), route_logits.T,
        expert_ids.T, w_gate, w_up, w_down,
    )


def solution(mesh):
    in_specs = (
        P(("grp", "ep"), None),
        P(),
        P(("grp", "ep")),
        P(("grp", "ep"), None),
        P(("grp", "ep"), None),
        P("ep", None, "tp"),
        P("ep", None, "tp"),
        P("ep", "tp", None),
    )
    out_specs = P(("grp", "ep"), None)
    return jax.shard_map(shards, mesh=mesh, in_specs=in_specs, out_specs=out_specs, check_vma=False)
```
